32 devices in a mesh: sp: 8 (over z, core), tp: 4 (over y, x).
Axes of the slice: x: 2, y: 2, z: 4, core: 2. Of those that a mesh axis runs over, the one named last changes fastest.
Arguments:
- skip_path_vectors: bfloat16 [2048, 2048], P('sp'), may hold values from -10 to 10
- asker_raw_scores: bfloat16 [2048, 2048], P('sp', 'tp'), may hold values from -6 to 6
- retain_raw_scores: bfloat16 [2048, 2048], P('sp', 'tp'), may hold values from -5.5 to 5.5
- memory_write_entries: bfloat16 [2048, 2048], P('sp', 'tp'), may hold values from -6 to 6
- emit_switch_scores: bfloat16 [2048, 2048], P('sp', 'tp'), may hold values from -6 to 6
- retain_minimum_share: float32 [2048], P('tp'), may hold values from 0.88 to 0.99990234
- extra_shrink_rate: float32 [16, 2048], P('tp', 'sp'), may hold values from -0.7 to 0
- lane_rescale_factor: float32 [128], replicated, may hold values from 0.1 to 1.9
- emit_projection_array: bfloat16 [2048, 2048], P('tp'), may hold values from -0.1875 to 0.1875
- specialist_rescale_factor: float32 [2048], replicated, may hold values from 0.1 to 1.9
- specialist_switch_proj: bfloat16 [8, 2048, 4096], P('sp', None, 'tp'), may hold values from -0.125 to 0.125
- specialist_raise_proj: bfloat16 [8, 2048, 4096], P('sp', None, 'tp'), may hold values from -0.125 to 0.125
- specialist_lower_proj: bfloat16 [8, 4096, 2048], P('sp', 'tp'), may hold values from -0.375 to 0.375
- specialist_choice_ids: int32 [2048, 2], P('sp'), may hold values from 0 to 7, all different within a row; in each aligned block of 256 rows (0 to 255, 256 to 511, ...) at most 96 rows name the same one
- cluster_chance: float32 [2048], P('sp'), may hold values from 0.1 to 0.6
- specialist_duo_scores: float32 [2048, 2], P('sp'), may hold values from -2 to 2
Outputs:
- mixed_out: bfloat16 [2048, 2048], P('sp', 'tp')
The draws below stay inside these ranges and needn't reach their ends.
Inputs may be any that keep to these rules, and one draw needn't show every extreme that they name: `specialist_choice_ids`: in each aligned block of 256 rows (the rows of one index of sp) no expert is named by more than 96 rows, a bound that some block reaches; the 2 ids of a row differ.
All inputs are finite; a program needn't handle non-finite values.
Results may differ from the reference program's by a relative error of at most 0.02.
Values may be sent and summed in bfloat16 or wider, within the bound.
A program may use at most 64 MiB of HBM per device.

```python
import math
import jax
import jax.numpy as jnp
import numpy as np
from jax import lax

D = 2048
SCAN_LANE_COUNT = 16
KEY_WIDTH_SIZE = 128
FFE = 4096
TOPK = 2
TOK_SP = 256
HG_W = 2048
EXPERTS = 8
SEQ = 2048
CAP = 96
N_SP = 8
N_TP = 4


def draw_skip_path_vectors(key, part):
    noise_key, row_key = jax.random.split(key)
    columns = jnp.arange(D, dtype=jnp.float32) / D
    noise = jnp.clip(jax.random.normal(noise_key, (SEQ, D), jnp.float32), -3.0, 3.0)
    col_scale = 10.0 ** (columns - 0.5)
    row_scale = 0.3 * jnp.exp(jax.random.uniform(row_key, (SEQ,), jnp.float32, math.log(0.3), math.log(3.0)))
    return (noise * row_scale[:, None] * col_scale[None, :]).astype(jnp.bfloat16)


def draw_retain_raw_scores(key, part):
    noise_key, shift_key = jax.random.split(key)
    blocks = SEQ // TOK_SP
    noise = jnp.clip(jax.random.normal(noise_key, (SEQ, HG_W), jnp.float32), -4.0, 4.0)
    shifts = jax.random.uniform(shift_key, (blocks, 1, 1), jnp.float32, -1.0, 1.0)
    return (noise.reshape(blocks, TOK_SP, HG_W) + shifts).reshape(SEQ, HG_W).astype(jnp.bfloat16)


def draw_retain_minimum_share(key, part):
    pick_key, slow_key, fast_key = jax.random.split(key, 3)
    slow_head = jax.random.randint(pick_key, (SCAN_LANE_COUNT,), 0, 2) > 0
    slow_gap = jnp.exp(jax.random.uniform(slow_key, (SCAN_LANE_COUNT, KEY_WIDTH_SIZE), jnp.float32, math.log(0.2), math.log(1.2))) / SEQ
    fast_gap = jnp.exp(jax.random.uniform(fast_key, (SCAN_LANE_COUNT, KEY_WIDTH_SIZE), jnp.float32, math.log(0.04), math.log(0.12)))
    gap = jnp.where(slow_head[:, None], slow_gap, fast_gap)
    return (1.0 - gap).reshape(HG_W).astype(jnp.float32)


def draw_extra_shrink_rate(key, part):
    where_key, size_key = jax.random.split(key)
    spots = jax.random.randint(where_key, (3,), 0, SEQ)
    strength = jnp.log(jax.random.uniform(size_key, (SCAN_LANE_COUNT, 3), jnp.float32, 0.5, 0.8))
    places = jnp.arange(SEQ)[None, None, :] == spots[None, :, None]
    return jnp.sum(jnp.where(places, strength[:, :, None], 0.0), axis=1).astype(jnp.float32)


def with_spikes(values, rng, source, target, blocks, factor):
    def block_of(position):
        return (jnp.arange(values.shape[position]) // (values.shape[position] // blocks)).reshape((-1,) + (1,) * (values.ndim - 1 - position))

    near = jax.random.permutation(rng, blocks)[block_of(target)]
    other_side = (block_of(target) + blocks // 2) % blocks
    return jnp.where((block_of(source) == near) | (block_of(source) == other_side), factor * values, values)


def steps_of(stream_key, dims, cuts, low, largest):
    gain, own = 1.0, jax.random.fold_in(stream_key, 6)
    for axis_at, parts in cuts:
        steps = jnp.exp(jax.random.uniform(jax.random.fold_in(own, axis_at), (parts,), jnp.float32, low / len(cuts), largest / len(cuts)))
        gain = gain * jnp.repeat(steps, dims[axis_at] // parts).reshape([-1 if axis == axis_at else 1 for axis in range(len(dims))])
    return gain


def routed_block(rng, own, number, rows, count, top, limit, skew):
    ranking = jax.random.permutation(rng, count)
    crowded, ordinary = shares(count, rows * top, limit, skew, True), shares(count, rows * top, limit, skew, False)
    places = jnp.arange(count)

    def named(sizes, rotation):
        used = int((sizes > 0).sum())
        fixed = max(1, used // 4)
        shifted = fixed + (places - fixed + rotation * (used - fixed)) % max(1, count - fixed)
        return jnp.zeros((count,), jnp.int32).at[ranking[jnp.where(places < fixed, places, shifted)]].set(jnp.asarray(sizes, jnp.int32))

    sizes = jnp.where(number % 4 == 0, named(crowded, number // 4), named(ordinary, number - number // 4 - 1))
    mixed = jax.random.permutation(jax.random.fold_in(own, 3), count)
    source_of, taker = mixed[0:count // 2 * 2:2], mixed[1:count // 2 * 2:2]
    margin = jnp.minimum(sizes[source_of] - 1, limit - sizes[taker]) // 2
    margin = jnp.where((source_of == ranking[0]) | (taker == ranking[0]) | (sizes[taker] == 0), 0, jnp.maximum(margin, 0))
    shifted = jax.random.randint(jax.random.fold_in(own, 4), (count // 2,), 0, 1 << 20) % (margin + 1)
    sizes = sizes.at[source_of].add(-shifted).at[taker].add(shifted)
    labels = jnp.searchsorted(jnp.cumsum(sizes), jnp.arange(rows * top), side="right").astype(jnp.int32)
    grid = labels.reshape(top, rows).T
    grid = grid[jax.random.permutation(jax.random.fold_in(own, 1), rows)]
    rotation = jax.random.randint(jax.random.fold_in(own, 2), (rows, 1), 0, top)
    return jnp.take_along_axis(grid, (jnp.arange(top)[None, :] + rotation) % top, axis=1)


def shares(amount, total, bound, slope, full):
    weights = [(1 << 20) // math.isqrt(standing ** slope) + 1 for standing in range(1, amount + 1)]
    largest = bound if full else min(bound, max(-(-total // amount), total * weights[0] // sum(weights)))
    least = 1 if total - largest >= amount - 1 else 0
    holding, surplus = [largest] + [least] * (amount - 1), total - largest - least * (amount - 1)
    while surplus > 0:
        candidates = [i for i in range(1, amount) if holding[i] < largest] or [i for i in range(1, amount) if holding[i] < bound]
        mass, remaining = sum([weights[i] for i in candidates]), surplus
        for i in candidates:
            addition = min(bound - holding[i], max(1, remaining * weights[i] // mass), surplus)
            holding[i] = holding[i] + addition
            surplus = surplus - addition
    return np.array(holding)


def scatter_about(rng, shape, width, most, shards=(), held_as=jnp.bfloat16):
    loudness = steps_of(rng, shape, shards, -0.22, 0.18) if shards else 1.0
    entries = jax.random.normal(rng, shape, jnp.float32) * width * loudness
    return jnp.minimum(jnp.maximum(entries, -most), most).astype(held_as)


def bell_draw_with(rng, shape, width, limit, pieces, heavy, kind=jnp.bfloat16):
    values = width * jax.random.normal(rng, shape, jnp.float32)
    if pieces:
        values = values * steps_of(rng, shape, pieces, -0.22, 0.18)
    return jnp.clip(with_spikes(values, jax.random.fold_in(rng, 3), *heavy), -limit, limit).astype(kind)


def setup_inputs(seed: int = 0) -> dict:
    streams_of = jax.random.split(jax.random.key(seed), 17)
    skip_path_vectors = draw_skip_path_vectors(jax.random.fold_in(streams_of[16], 71), 0)
    asker_raw_scores = scatter_about(streams_of[1], (SEQ, HG_W), 1.0, 6.0, ((0, 8), (1, 4)))
    retain_raw_scores = draw_retain_raw_scores(jax.random.fold_in(streams_of[16], 71), 0)
    memory_write_entries = scatter_about(streams_of[3], (SEQ, HG_W), 1.0, 6.0, ((0, 8), (1, 4)))
    emit_switch_scores = scatter_about(streams_of[4], (SEQ, HG_W), 1.0, 6.0, ((0, 8), (1, 4)))
    retain_minimum_share = draw_retain_minimum_share(jax.random.fold_in(streams_of[16], 71), 0)
    extra_shrink_rate = draw_extra_shrink_rate(jax.random.fold_in(streams_of[16], 71), 0)
    lane_rescale_factor = jnp.clip(1.0 + 0.18 * jax.random.normal(streams_of[7], (KEY_WIDTH_SIZE,), jnp.float32), 0.1, 1.9)
    emit_projection_array = bell_draw_with(streams_of[8], (HG_W, D), HG_W ** -0.5, 0.1875, ((0, 4),), (0, 1, 4, 2.0))
    specialist_rescale_factor = jnp.clip(1.0 + 0.18 * jax.random.normal(streams_of[9], (D,), jnp.float32), 0.1, 1.9)
    specialist_switch_proj = scatter_about(streams_of[10], (EXPERTS, D, FFE), D ** -0.5, 0.125, ((0, 8), (2, 4)))
    specialist_raise_proj = scatter_about(streams_of[11], (EXPERTS, D, FFE), D ** -0.5, 0.125, ((0, 8), (2, 4)))
    specialist_lower_proj = bell_draw_with(streams_of[12], (EXPERTS, FFE, D), (FFE // 8) ** -0.5, 0.375, ((0, 8), (1, 4)), (1, 2, 4, 2.0))
    specialist_choice_ids_keys = jax.random.split(jax.random.fold_in(streams_of[13], 1), SEQ // TOK_SP)
    specialist_choice_ids_turns = jax.random.permutation(jax.random.fold_in(streams_of[13], 3), SEQ // TOK_SP)
    specialist_choice_ids = jax.vmap(lambda own, number: routed_block(jax.random.fold_in(streams_of[13], 2), own, number, TOK_SP, EXPERTS, TOPK, CAP, 2))(specialist_choice_ids_keys, specialist_choice_ids_turns).reshape((SEQ, TOPK))
    cluster_chance = jnp.clip(0.1 + 0.5 * jax.random.uniform(streams_of[14], (SEQ,), jnp.float32) ** steps_of(streams_of[14], (SEQ,), ((0, 8),), -0.2, 0.2), 0.1, 0.6)
    specialist_duo_scores = scatter_about(streams_of[15], (SEQ, TOPK), 0.5, 2.0, ((0, 8),), jnp.float32)
    return dict(skip_path_vectors=skip_path_vectors, asker_raw_scores=asker_raw_scores, retain_raw_scores=retain_raw_scores, memory_write_entries=memory_write_entries, emit_switch_scores=emit_switch_scores, retain_minimum_share=retain_minimum_share, extra_shrink_rate=extra_shrink_rate, lane_rescale_factor=lane_rescale_factor, emit_projection_array=emit_projection_array, specialist_rescale_factor=specialist_rescale_factor, specialist_switch_proj=specialist_switch_proj, specialist_raise_proj=specialist_raise_proj, specialist_lower_proj=specialist_lower_proj, specialist_choice_ids=specialist_choice_ids, cluster_chance=cluster_chance, specialist_duo_scores=specialist_duo_scores)


EPS = 1e-06
PRECISE = lax.Precision.HIGHEST

def recurrence(queries, key_rows, values, shrink_log_rate):
    token_count_total = queries.shape[0]
    span_len = 64
    span_count = token_count_total // span_len
    causal = (jnp.arange(span_len)[:, None] >= jnp.arange(span_len)[None, :])[:, :, None, None]

    def advance(carried, inputs):
        query_span, key_span, value_span, decay_span = inputs
        cumulative = jnp.cumsum(decay_span, axis=0)
        spread = cumulative[:, None] - cumulative[None, :]
        factor = jnp.exp(jnp.where(causal, spread, -jnp.inf))
        scores = jnp.einsum('thd,shd,tshd->hts', query_span, key_span, factor, precision=PRECISE)
        inside = jnp.einsum('hts,shv->thv', scores, value_span, precision=PRECISE)
        outside = jnp.einsum('thd,hdv->thv', query_span * jnp.exp(cumulative), carried, precision=PRECISE)
        final_cum = cumulative[-1]
        written = jnp.einsum('shd,shv->hdv', key_span * jnp.exp(final_cum[None] - cumulative), value_span, precision=PRECISE)
        carried = jnp.exp(final_cum)[:, :, None] * carried + written
        return (carried, inside + outside)

    def split_spans(array):
        return array.reshape(span_count, span_len, SCAN_LANE_COUNT, KEY_WIDTH_SIZE)
    initial = jnp.zeros((SCAN_LANE_COUNT, KEY_WIDTH_SIZE, KEY_WIDTH_SIZE), jnp.float32)
    finished, output = lax.scan(advance, initial, tuple((split_spans(a) for a in (queries, key_rows, values, shrink_log_rate))))
    return output.reshape(token_count_total, SCAN_LANE_COUNT, KEY_WIDTH_SIZE)

def split_sum(left, right, groups):
    group_width = left.shape[1] // groups

    def add_group(running, group_idx):
        part_left = lax.dynamic_slice_in_dim(left, group_idx * group_width, group_width, 1)
        part_right = lax.dynamic_slice_in_dim(right, group_idx * group_width, group_width, 0)
        piece_sum = jnp.dot(part_left, part_right, preferred_element_type=jnp.float32)
        piece_sum = lax.optimization_barrier(piece_sum.astype(jnp.bfloat16)).astype(jnp.float32)
        return (running + piece_sum, None)
    zeros = jnp.zeros((left.shape[0], right.shape[1]), jnp.float32)
    total, finished = lax.scan(add_group, zeros, jnp.arange(groups, dtype=jnp.int32))
    return total

def experts_apply(normed, specialist_choice_ids, flat_weights, specialist_switch_proj, specialist_raise_proj, specialist_lower_proj):
    top_count = specialist_choice_ids.shape[1]
    flat_ids = specialist_choice_ids.reshape(-1)
    slot_limit = N_SP * CAP

    def one_expert(running, expert):
        ordering = jnp.argsort((flat_ids != expert).astype(jnp.int32), stable=True)[:slot_limit].astype(jnp.int32)
        chosen = flat_ids[ordering] == expert
        token_idx = (ordering // top_count).astype(jnp.int32)
        routed_rows = normed[token_idx]
        gate_acts = jnp.dot(routed_rows, specialist_switch_proj[expert], preferred_element_type=jnp.float32)
        up_acts = jnp.dot(routed_rows, specialist_raise_proj[expert], preferred_element_type=jnp.float32)
        hidden = (jax.nn.silu(gate_acts) * up_acts).astype(jnp.bfloat16)
        out_rows = split_sum(hidden, specialist_lower_proj[expert], N_TP).astype(jnp.bfloat16)
        scaled = jnp.where(chosen, flat_weights[ordering], 0.0)[:, None] * out_rows.astype(jnp.float32)
        return (running.at[token_idx].add(scaled), None)
    zeros = jnp.zeros(normed.shape, jnp.float32)
    total, finished = lax.scan(one_expert, zeros, jnp.arange(EXPERTS, dtype=jnp.int32))
    return total

def reference(skip_path_vectors, asker_raw_scores, retain_raw_scores, memory_write_entries, emit_switch_scores, retain_minimum_share, extra_shrink_rate, lane_rescale_factor, emit_projection_array, specialist_rescale_factor, specialist_switch_proj, specialist_raise_proj, specialist_lower_proj, specialist_choice_ids, cluster_chance, specialist_duo_scores):
    token_count_total = skip_path_vectors.shape[0]
    retain_share = retain_minimum_share + (1.0 - retain_minimum_share) * jax.nn.sigmoid(retain_raw_scores.astype(jnp.float32))
    shrink_log_rate = jnp.log(retain_share).reshape(token_count_total, SCAN_LANE_COUNT, KEY_WIDTH_SIZE) + extra_shrink_rate.T[:, :, None]
    key_rows = (1.0 - retain_share).reshape(token_count_total, SCAN_LANE_COUNT, KEY_WIDTH_SIZE)
    queries = jax.nn.silu(asker_raw_scores.astype(jnp.float32)).reshape(token_count_total, SCAN_LANE_COUNT, KEY_WIDTH_SIZE)
    values = memory_write_entries.astype(jnp.float32).reshape(token_count_total, SCAN_LANE_COUNT, KEY_WIDTH_SIZE)
    readout = recurrence(queries, key_rows, values, shrink_log_rate)
    normed_heads = readout * lax.rsqrt(lax.optimization_barrier(jnp.mean(readout * readout, axis=-1, keepdims=True)) + EPS)
    gated_out = normed_heads * lane_rescale_factor * jax.nn.silu(emit_switch_scores.astype(jnp.float32).reshape(token_count_total, SCAN_LANE_COUNT, KEY_WIDTH_SIZE))
    mixer_out = gated_out.reshape(token_count_total, SCAN_LANE_COUNT * KEY_WIDTH_SIZE).astype(jnp.bfloat16)
    resid = (skip_path_vectors.astype(jnp.float32) + split_sum(mixer_out, emit_projection_array, N_TP)).astype(jnp.bfloat16)
    wide_rows = resid.astype(jnp.float32)
    normed = (wide_rows * lax.rsqrt(lax.optimization_barrier(jnp.mean(wide_rows * wide_rows, axis=1, keepdims=True)) + EPS) * specialist_rescale_factor).astype(jnp.bfloat16)
    spread_logit = specialist_duo_scores[:, 0] - specialist_duo_scores[:, 1]
    weights = cluster_chance[:, None] * jnp.stack([jax.nn.sigmoid(spread_logit), jax.nn.sigmoid(-spread_logit)], axis=1)
    routed = experts_apply(normed, specialist_choice_ids, weights.reshape(-1), specialist_switch_proj, specialist_raise_proj, specialist_lower_proj)
    return (wide_rows + routed).astype(jnp.bfloat16)
```

```python
import functools

import jax
import jax.numpy as jnp
from jax import lax
from jax.experimental import pallas as pl
from jax.experimental.pallas import tpu as pltpu
from jax.sharding import PartitionSpec as P

EPS = 1e-06
PRECISE = lax.Precision.HIGHEST


MESH = pl.DeviceIdType.MESH
VMEM = pl.BlockSpec(memory_space=pltpu.VMEM)
VMEM_LIMIT = 60 * 1024 * 1024


def each(first, last, body):
    if last - first <= 8:
        for i in range(first, last):
            body(i)
    else:

        @pl.loop(first, last)
        def _(i):
            body(i)


def push(src, dst, send_sem, recv_sem, peer):
    return pltpu.make_async_remote_copy(
        src_ref=src,
        dst_ref=dst,
        send_sem=send_sem,
        recv_sem=recv_sem,
        device_id=peer,
        device_id_type=MESH,
    )


def state_kernel(sp_size, own_ref, out_ref, far_send, far_recv, near_send, near_recv):
    me = lax.axis_index("sp")
    pairs = sp_size // 2
    partner = me + 1 - 2 * lax.rem(me, 2)
    barrier = pltpu.get_barrier_semaphore()
    pl.semaphore_signal(barrier, inc=1, device_id={"sp": partner}, device_id_type=MESH)

    def far(d):
        return lax.rem(me + 2 * d, sp_size)

    def source(d):
        return lax.rem(me + sp_size - 2 * d, sp_size)

    def far_copy(d):
        return push(own_ref, out_ref.at[me], far_send.at[d], far_recv.at[d], {"sp": far(d)})

    def near_copy(d):
        block = own_ref if d is None else out_ref.at[source(d)]
        place = me if d is None else source(d)
        slot = 0 if d is None else d
        return push(
            block, out_ref.at[place], near_send.at[slot], near_recv.at[slot], {"sp": partner}
        )

    each(
        1,
        pairs,
        lambda d: pl.semaphore_signal(
            barrier, inc=1, device_id={"sp": far(d)}, device_id_type=MESH
        ),
    )
    pl.semaphore_wait(barrier, pairs)
    each(1, pairs, lambda d: far_copy(d).start())
    near_copy(None).start()

    def relay(d):
        far_copy(d).wait_recv()
        near_copy(d).start()

    each(1, pairs, relay)
    out_ref[me] = own_ref[...]
    near_copy(None).wait()

    def finish(d):
        far_copy(d).wait_send()
        near_copy(d).wait()

    each(1, pairs, finish)


def gather_states(packed):
    sp_size = lax.axis_size("sp")
    pairs = sp_size // 2
    dma = pltpu.SemaphoreType.DMA((pairs,))
    return pl.pallas_call(
        functools.partial(state_kernel, sp_size),
        out_shape=jax.ShapeDtypeStruct((sp_size,) + packed.shape, packed.dtype),
        in_specs=[VMEM],
        out_specs=VMEM,
        scratch_shapes=[dma, dma, dma, dma],
        compiler_params=pltpu.CompilerParams(collective_id=0, has_side_effects=True),
    )(packed)


def grid_of(tp_size):
    cols = max(d for d in range(1, tp_size + 1) if tp_size % d == 0 and d * d <= tp_size)
    return tp_size // cols, cols


def flip(index, mask):
    bit = 1
    while bit <= mask:
        if mask & bit:
            index = index + bit * (1 - 2 * lax.rem(index // bit, 2))
        bit *= 2
    return index


def partner_order(sp_size):
    unit = max(1, sp_size // 8)
    blocks = [list(range(i * unit, (i + 1) * unit)) for i in range(sp_size // unit)]
    if len(blocks) > 2:
        blocks = [blocks[0]] + blocks[2:] + [blocks[1]]
    return unit, [mask for block in blocks for mask in block]


class Scatter:
    def __init__(self, grid, part, got, comb, got2, s1, r1, s2, r2):
        self.grid = grid
        self.part, self.got, self.comb, self.got2 = part, got, comb, got2
        self.s1, self.r1, self.s2, self.r2 = s1, r1, s2, r2

    def sizes(self, u):
        rows, cols = self.grid.shape
        return (cols, rows) if u % 2 == 0 else (rows, cols)

    def place(self, u, i, j):
        n1, n2 = self.sizes(u)
        return i * n2 + j if u % 2 == 0 else j * n2 + i

    def first(self, u, a):
        n1, n2 = self.sizes(u)
        peer = self.grid.along_row(a) if u % 2 == 0 else self.grid.along_col(a)
        span = pl.ds(a * n2, n2)
        return push(
            self.part.at[u, span], self.got.at[u, span], self.s1.at[u, a], self.r1.at[u, a], {"tp": peer}
        )

    def second(self, u, b):
        peer = self.grid.along_col(b) if u % 2 == 0 else self.grid.along_row(b)
        return push(self.comb.at[u, b], self.got2.at[u, b], self.s2.at[u, b], self.r2.at[u, b], {"tp": peer})

    def start(self, u):
        for a in range(1, self.sizes(u)[0]):
            self.first(u, a).start()

    def middle(self, u):
        n1, n2 = self.sizes(u)
        for a in range(1, n1):
            self.first(u, a).wait_recv()
        for b in range(1, n2):
            self.comb[u, b] = self.near_sum(u, b).astype(jnp.bfloat16)
            self.second(u, b).start()

    def near_sum(self, u, b):
        n1, n2 = self.sizes(u)
        acc = self.part[u, b].astype(jnp.float32)
        for a in range(1, n1):
            acc += self.got[u, a * n2 + b].astype(jnp.float32)
        return acc

    def finish(self, u):
        acc = self.near_sum(u, 0)
        for b in range(1, self.sizes(u)[1]):
            self.second(u, b).wait_recv()
            acc += self.got2[u, b].astype(jnp.float32)
        return acc

    def drain(self, u):
        n1, n2 = self.sizes(u)
        for a in range(1, n1):
            self.first(u, a).wait_send()
        for b in range(1, n2):
            self.second(u, b).wait_send()


class Grid:
    def __init__(self, tp_size):
        self.shape = grid_of(tp_size)
        me = lax.axis_index("tp")
        self.row, self.col = me // self.shape[1], lax.rem(me, self.shape[1])

    def at(self, i, j):
        rows, cols = self.shape
        return lax.rem(self.row + j, rows) * cols + lax.rem(self.col + i, cols)

    def along_row(self, i):
        return self.at(i, 0)

    def along_col(self, j):
        return self.at(0, j)

    def from_row(self, i):
        return self.at(self.shape[1] - i, 0)

    def from_col(self, j):
        return self.at(0, self.shape[0] - j)


def expert_kernel(
    sp_size,
    tp_size,
    cap,
    mixer_ref,
    tok_ref,
    gain_ref,
    skip_hbm,
    proj_hbm,
    gate_hbm,
    up_hbm,
    down_hbm,
    out_ref,
    gate_w,
    up_w,
    down_w,
    proj_w,
    skip_v,
    pj_part,
    pj_got,
    pj_comb,
    pj_got2,
    resid_v,
    sq,
    oh0,
    oh1,
    slots_in,
    arr,
    part,
    got,
    comb,
    got2,
    hid,
    slots,
    ret,
    load_sem,
    pj_s1,
    pj_r1,
    pj_s2,
    pj_r2,
    sq_send,
    sq_recv,
    out_send,
    out_recv,
    own_row_send,
    own_row_recv,
    own_col_send,
    own_col_recv,
    relay_send,
    relay_recv,
    rs_s1,
    rs_r1,
    rs_s2,
    rs_r2,
    back_send,
    back_recv,
):
    my_s = lax.axis_index("sp")
    my_t = lax.axis_index("tp")
    grid = Grid(tp_size)
    grid_rows, grid_cols = grid.shape
    unit, masks = partner_order(sp_size)
    units = sp_size // unit
    unit_rows = unit * cap
    tokens, width = out_ref.shape
    model_width, hidden_width = gate_w.shape
    bf, f32 = jnp.bfloat16, jnp.float32
    half = tokens // 2

    my_cols = pl.ds(pl.multiple_of(my_t * width, width), width)
    pairs_in = (
        (proj_hbm, proj_w),
        (skip_hbm.at[:, my_cols], skip_v),
        (gate_hbm, gate_w),
        (up_hbm, up_w),
        (down_hbm, down_w),
    )
    loads = [pltpu.make_async_copy(src, dst, load_sem.at[i]) for i, (src, dst) in enumerate(pairs_in)]
    barrier = pltpu.get_barrier_semaphore()

    def tp_of(j):
        return lax.rem(my_t + j, tp_size)

    def sp_of(q):
        return flip(my_s, masks[q])

    each(
        1,
        tp_size,
        lambda j: pl.semaphore_signal(barrier, inc=1, device_id={"tp": tp_of(j)}, device_id_type=MESH),
    )
    for q in range(1, sp_size):
        pl.semaphore_signal(barrier, inc=1, device_id={"sp": sp_of(q)}, device_id_type=MESH)
    for load in loads:
        load.start()
    loads[0].wait()
    pl.semaphore_wait(barrier, tp_size + sp_size - 2)

    pj = Scatter(grid, pj_part, pj_got, pj_comb, pj_got2, pj_s1, pj_r1, pj_s2, pj_r2)

    def project(i, j):
        cols = pl.ds(pl.multiple_of(grid.at(i, j) * width, width), width)
        out = jnp.dot(mixer_ref[...], proj_w[:, cols], preferred_element_type=f32).astype(bf)
        pj_part[0, pj.place(0, i, j)] = out[:half]
        pj_part[1, pj.place(1, i, j)] = out[half:]

    targets = [(i, j) for i in range(grid_cols) for j in range(grid_rows)]
    for i, j in targets:
        if i > 0:
            project(i, j)
    pj.start(0)
    for i, j in targets:
        if i == 0 and j > 0:
            project(i, j)
    pj.start(1)
    project(0, 0)

    tok = tok_ref[...]
    lanes = -(-sp_size // 128) * 128
    lane = lax.broadcasted_iota(jnp.int32, (1, lanes), 1)
    base = jnp.zeros((1, lanes), f32)
    for q in range(sp_size):
        base = base + jnp.where(lane == sp_of(q), float(q * cap), 0.0)
    wide_lane = lax.broadcasted_iota(jnp.int32, (tokens, lanes), 1).astype(f32)
    mine = [(wide_lane == tok[:, j : j + 1]).astype(f32) for j in range(2)]
    row_id = lax.broadcasted_iota(jnp.int32, (tokens, tokens), 0)
    col_id = lax.broadcasted_iota(jnp.int32, (tokens, tokens), 1)
    before = (col_id < row_id).astype(f32).astype(bf)
    rank = jnp.dot(before, (mine[0] + mine[1]).astype(bf), preferred_element_type=f32) + base
    slot_ids = lax.broadcasted_iota(jnp.int32, (tokens, sp_size * cap), 1).astype(f32)
    for j, oh in enumerate((oh0, oh1)):
        spot = jnp.sum(rank * mine[j], axis=1, keepdims=True)
        oh[...] = (slot_ids == spot).astype(f32).astype(bf)
    weights = [
        tok[:, 2:3] * jax.nn.sigmoid(tok[:, 3:4] - tok[:, 4:5]),
        tok[:, 2:3] * jax.nn.sigmoid(tok[:, 4:5] - tok[:, 3:4]),
    ]

    pj.middle(0)
    pj.middle(1)
    loads[1].wait()
    total = jnp.concatenate([pj.finish(0), pj.finish(1)], axis=0)
    resid = (skip_v[...].astype(f32) + total).astype(bf)
    resid_v[...] = resid
    wide = resid.astype(f32)
    row_sums = jnp.sum(wide * wide, axis=1, keepdims=True)
    sq[0] = jnp.transpose(jnp.broadcast_to(row_sums, (tokens, 128)))[:8]

    def sq_copy(j):
        return push(sq.at[0], sq.at[j], sq_send.at[j], sq_recv.at[j], {"tp": tp_of(j)})

    each(1, tp_size, lambda j: sq_copy(j).start())
    scaled = wide * gain_ref[:, my_cols]
    each(1, tp_size, lambda j: sq_copy(j).wait())
    squares = jnp.sum(sq[...], axis=0)[0:1]
    squares = jnp.transpose(jnp.broadcast_to(squares, (128, tokens)))[:, 0:1]
    normed = (scaled * lax.rsqrt(squares / model_width + EPS)).astype(bf)

    both = oh0[...] + oh1[...]
    filled = lax.dot_general(
        both, normed, (((0,), (0,)), ((), ())), preferred_element_type=f32
    ).astype(bf)
    slots_in[...] = filled.reshape(sp_size, cap, width)
    arr[my_t, 0, pl.ds(0, cap)] = filled[:cap]

    def out_copy(q):
        dst = arr.at[my_t, q // unit, pl.ds((q % unit) * cap, cap)]
        return push(slots_in.at[q], dst, out_send.at[q], out_recv.at[q], {"sp": sp_of(q)})

    for q in range(1, sp_size):
        out_copy(q).start()

    def own_row(p, i):
        block = arr.at[my_t, p]
        return push(block, block, own_row_send.at[p, i], own_row_recv.at[p, i], {"tp": grid.along_row(i)})

    def own_col(p, j):
        block = arr.at[my_t, p]
        return push(block, block, own_col_send.at[p, j], own_col_recv.at[p, j], {"tp": grid.along_col(j)})

    def relay(p, i, j):
        if p % 2 == 0:
            block, peer = arr.at[grid.from_row(i), p], grid.along_col(j)
        else:
            block, peer = arr.at[grid.from_col(j), p], grid.along_row(i)
        return push(block, block, relay_send.at[p, i, j], relay_recv.at[p, i, j], {"tp": peer})

    def take(p):
        for i in range(unit):
            q = p * unit + i
            if q > 0:
                out_copy(q).wait_recv()
        for i in range(1, grid_cols):
            own_row(p, i).start()
        for j in range(1, grid_rows):
            own_col(p, j).start()

    def pass_on(p):
        if p % 2 == 0:
            for i in range(1, grid_cols):
                own_row(p, i).wait_recv()
                for j in range(1, grid_rows):
                    relay(p, i, j).start()
        else:
            for j in range(1, grid_rows):
                own_col(p, j).wait_recv()
                for i in range(1, grid_cols):
                    relay(p, i, j).start()

    def gathered(p):
        if p % 2 == 0:
            for j in range(1, grid_rows):
                own_col(p, j).wait_recv()
        else:
            for i in range(1, grid_cols):
                own_row(p, i).wait_recv()
        for i in range(1, grid_cols):
            for j in range(1, grid_rows):
                relay(p, i, j).wait_recv()

    rs = Scatter(grid, part, got, comb, got2, rs_s1, rs_r1, rs_s2, rs_r2)
    tile = min(256, hidden_width)

    def compute(g):
        pair = pl.ds(2 * g, 2)

        @pl.loop(0, hidden_width // tile)
        def _(f):
            cols = pl.ds(pl.multiple_of(f * tile, tile), tile)
            gate = jnp.zeros((2 * unit_rows, tile), f32)
            up = jnp.zeros((2 * unit_rows, tile), f32)
            for t in range(tp_size):
                x = arr[t, pair].reshape(2 * unit_rows, width)
                depth = slice(t * width, (t + 1) * width)
                gate += jnp.dot(x, gate_w[depth, cols], preferred_element_type=f32)
                up += jnp.dot(x, up_w[depth, cols], preferred_element_type=f32)
            hid[:, cols] = (gate * jax.nn.sigmoid(gate) * up).astype(bf)

        def lower(i, j):
            cols = pl.ds(pl.multiple_of(grid.at(i, j) * width, width), width)
            out = jnp.dot(hid[...], down_w[:, cols], preferred_element_type=f32).astype(bf)
            part[2 * g, rs.place(2 * g, i, j)] = out[:unit_rows]
            part[2 * g + 1, rs.place(2 * g + 1, i, j)] = out[unit_rows:]

        for i in range(1, grid_cols):
            for j in range(grid_rows):
                lower(i, j)
        rs.start(2 * g)
        for j in range(1, grid_rows):
            lower(0, j)
        rs.start(2 * g + 1)
        lower(0, 0)

    def back_copy(q):
        return push(slots.at[q], ret.at[q], back_send.at[q], back_recv.at[q], {"sp": sp_of(q)})

    def give_back(p):
        done = rs.finish(p).astype(bf)
        for i in range(unit):
            q = p * unit + i
            if q == 0:
                ret[0] = done[:cap]
            else:
                slots[q] = done[i * cap : (i + 1) * cap]
                back_copy(q).start()

    groups = units // 2
    take(0)
    take(1)
    pass_on(0)
    pass_on(1)
    for g in range(groups):
        now = (2 * g, 2 * g + 1)
        if g + 1 < groups:
            take(2 * g + 2)
            take(2 * g + 3)
        if g == 0:
            for load in loads[2:]:
                load.wait()
        for p in now:
            gathered(p)
        compute(g)
        if g + 1 < groups:
            pass_on(2 * g + 2)
            pass_on(2 * g + 3)
        if g >= 1:
            rs.middle(2 * g - 2)
            rs.middle(2 * g - 1)
        if g >= 2:
            give_back(2 * g - 4)
            give_back(2 * g - 3)
    last = units - 2
    rs.middle(last)
    rs.middle(last + 1)
    for p in range(max(0, units - 4), units):
        give_back(p)

    for q in range(1, sp_size):
        back_copy(q).wait_recv()
    returned = ret[...].reshape(sp_size * cap, width)
    mixed = resid_v[...].astype(f32)
    for j, oh in enumerate((oh0, oh1)):
        mixed += weights[j] * jnp.dot(oh[...], returned, preferred_element_type=f32)
    out_ref[...] = mixed.astype(bf)

    for u in range(2):
        pj.drain(u)
    for p in range(units):
        for i in range(1, grid_cols):
            own_row(p, i).wait_send()
            for j in range(1, grid_rows):
                relay(p, i, j).wait_send()
        for j in range(1, grid_rows):
            own_col(p, j).wait_send()
        rs.drain(p)
    for q in range(1, sp_size):
        out_copy(q).wait_send()
        back_copy(q).wait_send()


def run_experts(mixer_out, tok, gain, skip, projection, gate, up, down, cap):
    sp_size = lax.axis_size("sp")
    tp_size = lax.axis_size("tp")
    grid_rows, grid_cols = grid_of(tp_size)
    side = max(grid_rows, grid_cols)
    tokens, model_width = skip.shape
    width = model_width // tp_size
    hidden_width = gate.shape[1]
    unit, masks = partner_order(sp_size)
    units = sp_size // unit
    rows = unit * cap
    half = tokens // 2
    bf, f32 = jnp.bfloat16, jnp.float32
    dma = pltpu.SemaphoreType.DMA
    anywhere = pl.BlockSpec(memory_space=pl.ANY)
    vmem = pltpu.VMEM
    return pl.pallas_call(
        functools.partial(expert_kernel, sp_size, tp_size, cap),
        out_shape=jax.ShapeDtypeStruct((tokens, width), bf),
        in_specs=[VMEM] * 3 + [anywhere] * 5,
        out_specs=VMEM,
        scratch_shapes=[
            vmem(gate.shape, bf),
            vmem(up.shape, bf),
            vmem(down.shape, bf),
            vmem(projection.shape, bf),
            vmem((tokens, width), bf),
            vmem((2, tp_size, half, width), bf),
            vmem((2, tp_size, half, width), bf),
            vmem((2, side, half, width), bf),
            vmem((2, side, half, width), bf),
            vmem((tokens, width), bf),
            vmem((tp_size, 8, tokens), f32),
            vmem((tokens, sp_size * cap), bf),
            vmem((tokens, sp_size * cap), bf),
            vmem((sp_size, cap, width), bf),
            vmem((tp_size, units, rows, width), bf),
            vmem((units, tp_size, rows, width), bf),
            vmem((units, tp_size, rows, width), bf),
            vmem((units, side, rows, width), bf),
            vmem((units, side, rows, width), bf),
            vmem((2 * rows, hidden_width), bf),
            vmem((sp_size, cap, width), bf),
            vmem((sp_size, cap, width), bf),
            dma((5,)),
            dma((2, side)),
            dma((2, side)),
            dma((2, side)),
            dma((2, side)),
            dma((tp_size,)),
            dma((tp_size,)),
            dma((sp_size,)),
            dma((sp_size,)),
            dma((units, grid_cols)),
            dma((units, grid_cols)),
            dma((units, grid_rows)),
            dma((units, grid_rows)),
            dma((units, grid_cols, grid_rows)),
            dma((units, grid_cols, grid_rows)),
            dma((units, side)),
            dma((units, side)),
            dma((units, side)),
            dma((units, side)),
            dma((sp_size,)),
            dma((sp_size,)),
        ],
        compiler_params=pltpu.CompilerParams(
            collective_id=1, has_side_effects=True, vmem_limit_bytes=VMEM_LIMIT
        ),
    )(mixer_out, tok, gain, skip, projection, gate, up, down)


def carry_states(totals, own_state):
    lanes, depth = totals.shape
    sp_size = lax.axis_size("sp")
    place = lax.axis_index("sp")
    pad = -lanes % 16
    packed = jnp.concatenate(
        [
            own_state.astype(jnp.bfloat16).reshape(lanes * depth, depth),
            totals.astype(jnp.bfloat16),
            jnp.zeros((pad, depth), jnp.bfloat16),
        ]
    )
    gathered = gather_states(packed)
    states = gathered[:, : lanes * depth].reshape(sp_size, lanes, depth, depth)
    shrinks = gathered[:, lanes * depth : lanes * depth + lanes].astype(jnp.float32)
    factor = jnp.ones((lanes, depth), jnp.float32)
    carried = jnp.zeros((lanes, depth, depth), jnp.float32)
    for lap in reversed(range(sp_size)):
        earlier = lap < place
        held = states[lap].astype(jnp.float32) * factor[:, :, None]
        carried = carried + jnp.where(earlier, held, 0.0)
        factor = jnp.where(earlier, factor * shrinks[lap], factor)
    return carried


def shards(
    skip_path_vectors,
    asker_raw_scores,
    retain_raw_scores,
    memory_write_entries,
    emit_switch_scores,
    retain_minimum_share,
    extra_shrink_rate,
    lane_rescale_factor,
    emit_projection_array,
    specialist_rescale_factor,
    specialist_switch_proj,
    specialist_raise_proj,
    specialist_lower_proj,
    specialist_choice_ids,
    cluster_chance,
    specialist_duo_scores,
):
    token_count_total = skip_path_vectors.shape[0]
    model_width = skip_path_vectors.shape[1]
    head_depth = lane_rescale_factor.shape[0]
    lanes_on_device = extra_shrink_rate.shape[0]
    retain_share = retain_minimum_share + (1.0 - retain_minimum_share) * jax.nn.sigmoid(
        retain_raw_scores.astype(jnp.float32)
    )
    retain_share = retain_share.reshape(token_count_total, lanes_on_device, head_depth)
    shrink_log_rate = jnp.log(retain_share) + extra_shrink_rate.T[:, :, None]
    key_rows = 1.0 - retain_share
    queries = jax.nn.silu(asker_raw_scores.astype(jnp.float32)).reshape(
        token_count_total, lanes_on_device, head_depth
    )
    values = memory_write_entries.astype(jnp.float32).reshape(
        token_count_total, lanes_on_device, head_depth
    )
    cumulative = jnp.cumsum(shrink_log_rate, axis=0)
    query_tilde = queries * jnp.exp(cumulative)
    key_tilde = key_rows * jnp.exp(-cumulative)
    causal = jnp.arange(token_count_total)[:, None] >= jnp.arange(token_count_total)[None, :]
    scores = jnp.einsum("thd,shd->hts", query_tilde, key_tilde, precision=PRECISE)
    scores = jnp.where(causal[None], scores, 0.0)
    inside = jnp.einsum("hts,shv->thv", scores, values, precision=PRECISE)
    totals = jnp.exp(cumulative[-1])
    own_state = jnp.einsum("shd,shv->hdv", key_tilde * totals[None], values, precision=PRECISE)
    carried = carry_states(totals, own_state)
    outside = jnp.einsum("thd,hdv->thv", query_tilde, carried, precision=PRECISE)
    readout = inside + outside
    normed_heads = readout * lax.rsqrt(jnp.mean(readout * readout, axis=-1, keepdims=True) + EPS)
    gated_out = (
        normed_heads
        * lane_rescale_factor
        * jax.nn.silu(
            emit_switch_scores.astype(jnp.float32).reshape(
                token_count_total, lanes_on_device, head_depth
            )
        )
    )
    mixer_out = gated_out.reshape(token_count_total, lanes_on_device * head_depth).astype(
        jnp.bfloat16
    )
    tp_size = lax.axis_size("tp")
    sp_size = lax.axis_size("sp")
    experts = sp_size
    top_count = specialist_choice_ids.shape[1]
    capacity = -(-3 * token_count_total * top_count // (2 * experts))
    capacity = -(-capacity // 16) * 16
    tok = jnp.concatenate(
        [specialist_choice_ids.astype(jnp.float32), cluster_chance[:, None], specialist_duo_scores], axis=1
    )
    return run_experts(
        mixer_out,
        tok,
        specialist_rescale_factor[None, :],
        skip_path_vectors,
        emit_projection_array,
        specialist_switch_proj[0],
        specialist_raise_proj[0],
        specialist_lower_proj[0],
        capacity,
    )


def solution(mesh):
    return jax.shard_map(
        shards,
        mesh=mesh,
        in_specs=(
            P("sp", None),
            P("sp", "tp"),
            P("sp", "tp"),
            P("sp", "tp"),
            P("sp", "tp"),
            P("tp"),
            P("tp", "sp"),
            P(),
            P("tp", None),
            P(),
            P("sp", None, "tp"),
            P("sp", None, "tp"),
            P("sp", "tp", None),
            P("sp", None),
            P("sp"),
            P("sp", None),
        ),
        out_specs=P("sp", "tp"),
        check_vma=False,
    )
```

```python
import functools

import jax
import jax.numpy as jnp
from jax import lax
from jax.experimental import pallas as pl
from jax.experimental.pallas import tpu as pltpu
from jax.sharding import PartitionSpec as P

EPS = 1e-06
MESH = pl.DeviceIdType.MESH
VMEM = pl.BlockSpec(memory_space=pltpu.VMEM)
VMEM_LIMIT = 56 * 1024 * 1024


def each(first, last, body):
    if last - first <= 8:
        for i in range(first, last):
            body(i)
    else:

        @pl.loop(first, last)
        def _(i):
            body(i)


def push(src, dst, send_sem, recv_sem, peer):
    return pltpu.make_async_remote_copy(
        src_ref=src,
        dst_ref=dst,
        send_sem=send_sem,
        recv_sem=recv_sem,
        device_id=peer,
        device_id_type=MESH,
    )


def grid_of(tp_size):
    cols = max(d for d in range(1, tp_size + 1) if tp_size % d == 0 and d * d <= tp_size)
    return tp_size // cols, cols


def flip(index, mask):
    bit = 1
    while bit <= mask:
        if mask & bit:
            index = index + bit * (1 - 2 * lax.rem(index // bit, 2))
        bit *= 2
    return index


def partner_order(sp_size):
    unit = sp_size // 8
    return unit, [k * unit + i for k in (2, 4, 3, 5, 6, 7, 0, 1) for i in range(unit)]


class Scatter:
    def __init__(self, grid, part, got, comb, got2, s1, r1, s2, r2):
        self.grid = grid
        self.part, self.got, self.comb, self.got2 = part, got, comb, got2
        self.s1, self.r1, self.s2, self.r2 = s1, r1, s2, r2

    def sizes(self, u):
        rows, cols = self.grid.shape
        return (cols, rows) if u % 2 == 0 else (rows, cols)

    def place(self, u, i, j):
        n1, n2 = self.sizes(u)
        return i * n2 + j if u % 2 == 0 else j * n2 + i

    def first(self, u, a):
        n1, n2 = self.sizes(u)
        peer = self.grid.along_row(a) if u % 2 == 0 else self.grid.along_col(a)
        span = pl.ds(a * n2, n2)
        return push(
            self.part.at[u, span], self.got.at[u, span], self.s1.at[u, a], self.r1.at[u, a], {"tp": peer}
        )

    def second(self, u, b):
        peer = self.grid.along_col(b) if u % 2 == 0 else self.grid.along_row(b)
        return push(self.comb.at[u, b], self.got2.at[u, b], self.s2.at[u, b], self.r2.at[u, b], {"tp": peer})

    def start(self, u):
        for a in range(1, self.sizes(u)[0]):
            self.first(u, a).start()

    def middle(self, u):
        n1, n2 = self.sizes(u)
        for a in range(1, n1):
            self.first(u, a).wait_recv()
        for b in range(1, n2):
            self.comb[u, b] = self.near_sum(u, b).astype(jnp.bfloat16)
            self.second(u, b).start()

    def near_sum(self, u, b):
        n1, n2 = self.sizes(u)
        acc = self.part[u, b].astype(jnp.float32)
        for a in range(1, n1):
            acc += self.got[u, a * n2 + b].astype(jnp.float32)
        return acc

    def finish(self, u):
        acc = self.near_sum(u, 0)
        for b in range(1, self.sizes(u)[1]):
            self.second(u, b).wait_recv()
            acc += self.got2[u, b].astype(jnp.float32)
        return acc

    def drain(self, u):
        n1, n2 = self.sizes(u)
        for a in range(1, n1):
            self.first(u, a).wait_send()
        for b in range(1, n2):
            self.second(u, b).wait_send()


class Grid:
    def __init__(self, tp_size):
        self.shape = grid_of(tp_size)
        me = lax.axis_index("tp")
        self.row, self.col = me // self.shape[1], lax.rem(me, self.shape[1])

    def at(self, i, j):
        rows, cols = self.shape
        return lax.rem(self.row + j, rows) * cols + lax.rem(self.col + i, cols)

    def along_row(self, i):
        return self.at(i, 0)

    def along_col(self, j):
        return self.at(0, j)

    def from_row(self, i):
        return self.at(self.shape[1] - i, 0)

    def from_col(self, j):
        return self.at(0, self.shape[0] - j)


def split_bf(x):
    high = x.astype(jnp.bfloat16)
    return high, (x - high.astype(jnp.float32)).astype(jnp.bfloat16)


def over_rows(a, b):
    return lax.dot_general(a, b, (((0,), (0,)), ((), ())), preferred_element_type=jnp.float32)


def over_lanes(a, b):
    return lax.dot_general(a, b, (((1,), (1,)), ((), ())), preferred_element_type=jnp.float32)


class Mixer:
    def __init__(self, heads, depth, sp_size, refs):
        (
            self.ask,
            self.keep,
            self.val,
            self.emit,
            self.key_v,
            self.cum_v,
            self.read_v,
            self.gate_v,
            self.qx_v,
            self.own,
            self.par,
            self.chip_own,
            self.chip_in,
            self.carry_f,
            self.carry_own,
            self.carry_par,
            self.mixed,
            self.pair_send,
            self.pair_recv,
            self.chip_send,
            self.chip_recv,
            self.carry_send,
            self.carry_recv,
        ) = refs
        self.heads, self.depth = heads, depth
        self.half = depth // 2
        self.body = heads * self.half
        self.chips = sp_size // 2
        self.me = lax.axis_index("sp")
        self.core = lax.rem(self.me, 2)
        self.chip = self.me // 2
        self.partner = self.me + 1 - 2 * self.core
        self.tokens = self.ask.shape[0]
        self.chunk = self.tokens // 2

    def lanes_of(self, h):
        return slice(h * self.depth, (h + 1) * self.depth)

    def rows_of(self, c):
        return slice(c * self.chunk, (c + 1) * self.chunk)

    def pair_copy(self):
        return push(self.own, self.par, self.pair_send, self.pair_recv, {"sp": self.partner})

    def chip_copy(self, d):
        return push(
            self.chip_own, self.chip_in.at[d], self.chip_send.at[d], self.chip_recv.at[d], {"sp": self.me + 2 * d}
        )

    def carry_copy(self):
        return push(self.carry_own, self.carry_par, self.carry_send, self.carry_recv, {"sp": self.partner})

    def states(self, share_ref, tok):
        f32, bf = jnp.float32, jnp.bfloat16
        n = self.chunk
        lower = lax.broadcasted_iota(jnp.int32, (n, n), 1) <= lax.broadcasted_iota(jnp.int32, (n, n), 0)
        lower = lower.astype(f32).astype(bf)
        for h in range(self.heads):
            lanes = self.lanes_of(h)
            share = share_ref[:, lanes]
            kept = share + (1.0 - share) * jax.nn.sigmoid(self.keep[:, lanes].astype(f32))
            key = 1.0 - kept
            decay = jnp.log(kept) + tok[:, 5 + h : 6 + h]
            self.key_v[:, lanes] = key
            parts, ends = [], []
            for c in range(2):
                rows = self.rows_of(c)
                d1, d2 = split_bf(decay[rows])
                d3 = (decay[rows] - d1.astype(f32) - d2.astype(f32)).astype(bf)
                sums = jnp.dot(lower, jnp.concatenate([d1, d2, d3], axis=1), preferred_element_type=f32)
                w = self.depth
                cum = sums[:, :w] + sums[:, w : 2 * w] + sums[:, 2 * w :]
                self.cum_v[rows, lanes] = cum
                end = cum[n - 1 : n]
                ends.append(end)
                late = jnp.concatenate(split_bf(key[rows] * jnp.exp(end - cum)), axis=1)
                state = over_rows(self.val[rows, lanes], late)
                parts.append(state[:, :w] + state[:, w:])
            self.read_v[self.rows_of(1), lanes] = parts[0]
            state = (parts[0] * jnp.exp(ends[1]) + parts[1]).astype(bf)
            total = jnp.exp(ends[0] + ends[1]).astype(bf)
            for k in range(2):
                self.own[k, h * self.half : (h + 1) * self.half] = state[k * self.half : (k + 1) * self.half]
                self.own[k, self.body + h : self.body + h + 1] = total

    def total_of(self, ref, h):
        return ref[self.body + h : self.body + h + 1].astype(jnp.float32)

    def join(self):
        f32, bf = jnp.float32, jnp.bfloat16
        self.pair_copy().wait_recv()
        own, par = self.own.at[self.core], self.par.at[self.core]
        odd = self.core == 1
        for h in range(self.heads):
            rows = slice(h * self.half, (h + 1) * self.half)
            mine, other = own[rows].astype(f32), par[rows].astype(f32)
            mine_t, other_t = self.total_of(own, h), self.total_of(par, h)
            joined = jnp.where(odd, other * mine_t + mine, mine * other_t + other)
            self.chip_own[rows] = joined.astype(bf)
            self.chip_own[self.body + h : self.body + h + 1] = (mine_t * other_t).astype(bf)
        for d in reversed(range(1, self.chips)):

            @pl.when(self.chip + d < self.chips)
            def _(d=d):
                self.chip_copy(d).start()

    def inside(self, gain_ref):
        f32, bf = jnp.float32, jnp.bfloat16
        n = self.chunk
        causal = lax.broadcasted_iota(jnp.int32, (n, n), 1) <= lax.broadcasted_iota(jnp.int32, (n, n), 0)
        for h in range(self.heads):
            lanes = self.lanes_of(h)
            first_end = None
            for c in range(2):
                rows = self.rows_of(c)
                raw = self.ask[rows, lanes].astype(f32)
                query = raw * jax.nn.sigmoid(raw)
                cum, key = self.cum_v[rows, lanes], self.key_v[rows, lanes]
                middle = cum[n // 2 - 1 : n // 2]
                q_mid = query * jnp.exp(cum - middle)
                q1, q2 = split_bf(q_mid)
                k1, k2 = split_bf(key * jnp.exp(middle - cum))
                scores = over_lanes(
                    jnp.concatenate([q1, q2, q1], axis=1), jnp.concatenate([k1, k1, k2], axis=1)
                )
                scores = jnp.where(causal, scores, 0.0)
                values = self.val[rows, lanes]
                read = jnp.dot(
                    jnp.concatenate(split_bf(scores), axis=1),
                    jnp.concatenate([values, values], axis=0),
                    preferred_element_type=f32,
                )
                q_start = query * jnp.exp(cum)
                if c == 0:
                    first_end = cum[n - 1 : n]
                else:
                    early = self.read_v[rows, lanes]
                    q_pair = jnp.concatenate(split_bf(q_start), axis=1)
                    e1 = early.astype(bf)
                    read += over_lanes(q_pair, jnp.concatenate([e1, e1], axis=1))
                    q_start = q_start * jnp.exp(first_end)
                self.read_v[rows, lanes] = read
                w = self.depth
                self.qx_v[rows, 2 * h * w : 2 * (h + 1) * w] = jnp.concatenate(split_bf(q_start), axis=1)
                raw = self.emit[rows, lanes].astype(f32)
                self.gate_v[rows, lanes] = raw * jax.nn.sigmoid(raw) * gain_ref[...]

    def carry(self):
        f32, bf = jnp.float32, jnp.bfloat16
        self.carry_f[...] = jnp.zeros_like(self.carry_f)
        shape = (1, self.depth)
        factors = [jnp.ones(shape, f32) for _ in range(self.heads)]
        for d in range(1, self.chips):
            there = self.chip >= d

            @pl.when(there)
            def _(d=d):
                self.chip_copy(d).wait_recv()
                for h in range(self.heads):
                    rows = slice(h * self.half, (h + 1) * self.half)
                    scale = jnp.ones(shape, f32)
                    for e in range(1, d):
                        scale = scale * self.total_of(self.chip_in.at[e], h)
                    self.carry_f[rows] += scale * self.chip_in[d, rows].astype(f32)

        self.carry_own[...] = self.carry_f[...].astype(bf)
        self.carry_copy().start()

    def outside(self):
        f32, bf = jnp.float32, jnp.bfloat16
        self.carry_copy().wait_recv()
        odd = self.core == 1
        for h in range(self.heads):
            lanes = self.lanes_of(h)
            rows = slice(h * self.half, (h + 1) * self.half)
            mine, other = self.carry_own[rows].astype(f32), self.carry_par[rows].astype(f32)
            low, high = jnp.where(odd, other, mine), jnp.where(odd, mine, other)
            start = jnp.concatenate([low, high], axis=0)
            before = jnp.concatenate([self.par[0, rows], self.par[1, rows]], axis=0).astype(f32)
            later = start * self.total_of(self.par.at[0], h) + before
            state = jnp.where(odd, later, start).astype(bf)
            w = self.depth
            read = self.read_v[:, lanes] + over_lanes(
                self.qx_v[:, 2 * h * w : 2 * (h + 1) * w], jnp.concatenate([state, state], axis=1)
            )
            level = jnp.mean(read * read, axis=1, keepdims=True)
            self.mixed[:, lanes] = (read * lax.rsqrt(level + EPS) * self.gate_v[:, lanes]).astype(bf)

    def drain(self):
        self.pair_copy().wait_send()
        self.carry_copy().wait_send()
        for d in range(1, self.chips):

            @pl.when(self.chip + d < self.chips)
            def _(d=d):
                self.chip_copy(d).wait_send()


def layer_kernel(
    sp_size,
    tp_size,
    cap,
    heads,
    depth,
    ids_ref,
    chance_ref,
    duo_ref,
    shrink_ref,
    gain_ref,
    share_ref,
    lane_gain_ref,
    ask_hbm,
    keep_hbm,
    val_hbm,
    emit_hbm,
    skip_hbm,
    proj_hbm,
    gate_hbm,
    up_hbm,
    down_hbm,
    out_ref,
    resid_v,
    *scratch,
):
    mixer_refs, scratch = scratch[:23], scratch[23:]
    (
    gate_w,
    up_w,
    down_w,
    proj_w,
    skip_v,
    pj_part,
    pj_got,
    pj_comb,
    pj_got2,
    tok_v,
    sq,
    scale_out,
    scale_in,
    scale_v,
    oh0,
    oh1,
    slots_in,
    arr,
    part,
    got,
    comb,
    got2,
    hid,
    slots,
    ret,
    load_sem,
    pj_s1,
    pj_r1,
    pj_s2,
    pj_r2,
    sq_send,
    sq_recv,
    scale_send,
    scale_recv,
    out_send,
    out_recv,
    own_row_send,
    own_row_recv,
    own_col_send,
    own_col_recv,
    relay_send,
    relay_recv,
    rs_s1,
    rs_r1,
    rs_s2,
    rs_r2,
    back_send,
    back_recv,
    ) = scratch
    my_s = lax.axis_index("sp")
    my_t = lax.axis_index("tp")
    grid = Grid(tp_size)
    grid_rows, grid_cols = grid.shape
    unit, masks = partner_order(sp_size)
    units = sp_size // unit
    unit_rows = unit * cap
    tokens, width = out_ref.shape
    model_width, hidden_width = gate_w.shape
    bf, f32 = jnp.bfloat16, jnp.float32
    pj_units, pj_rows = pj_part.shape[0], pj_part.shape[2]

    mix = Mixer(heads, depth, sp_size, mixer_refs)
    my_cols = pl.ds(pl.multiple_of(my_t * width, width), width)
    pairs_in = (
        (keep_hbm, mix.keep),
        (val_hbm, mix.val),
        (ask_hbm, mix.ask),
        (emit_hbm, mix.emit),
        (proj_hbm, proj_w),
        (skip_hbm.at[:, my_cols], skip_v),
        (gate_hbm, gate_w),
        (up_hbm, up_w),
        (down_hbm, down_w),
    )
    loads = [pltpu.make_async_copy(src, dst, load_sem.at[i]) for i, (src, dst) in enumerate(pairs_in)]
    barrier = pltpu.get_barrier_semaphore()

    def tp_of(j):
        return lax.rem(my_t + j, tp_size)

    def sp_of(q):
        return flip(my_s, masks[q])

    others = [q for q in range(sp_size) if masks[q]]
    home = masks.index(0)

    each(
        1,
        tp_size,
        lambda j: pl.semaphore_signal(barrier, inc=1, device_id={"tp": tp_of(j)}, device_id_type=MESH),
    )
    for q in others:
        pl.semaphore_signal(barrier, inc=1, device_id={"sp": sp_of(q)}, device_id_type=MESH)
    for load in loads:
        load.start()
    tok_v[...] = jnp.zeros_like(tok_v)
    tok_v[0:2] = ids_ref[...].astype(f32)
    tok_v[2:3] = chance_ref[...]
    tok_v[3:5] = duo_ref[...]
    tok_v[5 : 5 + heads] = shrink_ref[...]
    tok = jnp.transpose(tok_v[...])
    with jax.named_scope("states"):
        loads[0].wait()
        loads[1].wait()
        mix.states(share_ref, tok)
    with jax.named_scope("barrier"):
        pl.semaphore_wait(barrier, tp_size + sp_size - 2)
    mix.pair_copy().start()
    lanes = -(-sp_size // 128) * 128
    lane = lax.broadcasted_iota(jnp.int32, (1, lanes), 1)
    base = jnp.zeros((1, lanes), f32)
    for q in range(sp_size):
        base = base + jnp.where(lane == sp_of(q), float(q * cap), 0.0)
    wide_lane = lax.broadcasted_iota(jnp.int32, (tokens, lanes), 1).astype(f32)
    mine = [(wide_lane == tok[:, j : j + 1]).astype(f32) for j in range(2)]
    row_id = lax.broadcasted_iota(jnp.int32, (tokens, tokens), 0)
    col_id = lax.broadcasted_iota(jnp.int32, (tokens, tokens), 1)
    before = (col_id < row_id).astype(f32).astype(bf)
    rank = jnp.dot(before, (mine[0] + mine[1]).astype(bf), preferred_element_type=f32) + base
    slot_ids = lax.broadcasted_iota(jnp.int32, (tokens, sp_size * cap), 1).astype(f32)
    for j, oh in enumerate((oh0, oh1)):
        spot = jnp.sum(rank * mine[j], axis=1, keepdims=True)
        oh[...] = (slot_ids == spot).astype(f32).astype(bf)
    weights = [
        tok[:, 2:3] * jax.nn.sigmoid(tok[:, 3:4] - tok[:, 4:5]),
        tok[:, 2:3] * jax.nn.sigmoid(tok[:, 4:5] - tok[:, 3:4]),
    ]

    with jax.named_scope("join"):
        mix.join()
        loads[2].wait()
        loads[3].wait()
    with jax.named_scope("inside"):
        mix.inside(lane_gain_ref)
    with jax.named_scope("carry"):
        mix.carry()
        loads[4].wait()
    with jax.named_scope("outside"):
        mix.outside()

    pj = Scatter(grid, pj_part, pj_got, pj_comb, pj_got2, pj_s1, pj_r1, pj_s2, pj_r2)

    def project(i, j):
        cols = pl.ds(pl.multiple_of(grid.at(i, j) * width, width), width)
        out = jnp.dot(mix.mixed[...], proj_w[:, cols], preferred_element_type=f32).astype(bf)
        for u in range(pj_units):
            pj_part[u, pj.place(u, i, j)] = out[u * pj_rows : (u + 1) * pj_rows]

    targets = [(i, j) for i in range(grid_cols) for j in range(grid_rows)]
    for i, j in targets:
        if i > 0:
            project(i, j)
    for i, j in targets:
        if i == 0 and j > 0:
            project(i, j)
    for u in range(pj_units):
        pj.start(u)
    project(0, 0)

    with jax.named_scope("pj_middle"):
        for u in range(pj_units):
            pj.middle(u)
        loads[5].wait()
    with jax.named_scope("pj_finish"):
        total = jnp.concatenate([pj.finish(u) for u in range(pj_units)], axis=0)
    resid = (skip_v[...].astype(f32) + total).astype(bf)
    resid_v[...] = resid
    wide = resid.astype(f32)
    scaled = (wide * gain_ref[:, my_cols]).astype(bf)

    both = oh0[...] + oh1[...]
    filled = lax.dot_general(
        both, scaled, (((0,), (0,)), ((), ())), preferred_element_type=f32
    ).astype(bf)
    slots_in[...] = filled.reshape(sp_size, cap, width)
    arr[my_t, home // unit, pl.ds((home % unit) * cap, cap)] = filled[home * cap : (home + 1) * cap]

    def out_copy(q):
        dst = arr.at[my_t, q // unit, pl.ds((q % unit) * cap, cap)]
        return push(slots_in.at[q], dst, out_send.at[q], out_recv.at[q], {"sp": sp_of(q)})

    def send_out(p):
        for q in range(p * unit, (p + 1) * unit):
            if q != home:
                out_copy(q).start()

    def sq_copy(j):
        return push(sq.at[0], sq.at[j], sq_send.at[j], sq_recv.at[j], {"tp": tp_of(j)})

    def scale_copy(q):
        return push(
            scale_out.at[q], scale_in.at[q], scale_send.at[q], scale_recv.at[q], {"sp": sp_of(q)}
        )

    def start_squares():
        row_sums = jnp.sum(wide * wide, axis=1, keepdims=True)
        sq[0] = jnp.transpose(jnp.broadcast_to(row_sums, (tokens, 128)))[:8]
        each(1, tp_size, lambda j: sq_copy(j).start())

    def send_scales():
        each(1, tp_size, lambda j: sq_copy(j).wait_recv())
        scale = lax.rsqrt(jnp.sum(sq[...], axis=0) / model_width + EPS)
        s1, s2 = split_bf(scale)
        s3 = (scale - s1.astype(f32) - s2.astype(f32)).astype(bf)
        picked = sum(jnp.dot(term, both, preferred_element_type=f32) for term in (s1, s2, s3))
        for q in range(sp_size):
            dst = scale_in if q == home else scale_out
            dst[q, :, 0:cap] = picked[:, q * cap : (q + 1) * cap]
        for q in others:
            scale_copy(q).start()

    def column_of(g):
        cols = []
        for q in range(2 * g * unit, 2 * (g + 1) * unit):
            if q != home:
                scale_copy(q).wait_recv()
            tall = jnp.transpose(jnp.broadcast_to(scale_in[q, 0:1], (128, 128)))
            cols.append(tall[:cap])
        scale_v[...] = jnp.concatenate(cols, axis=0)

    def own_row(p, i):
        block = arr.at[my_t, p]
        return push(block, block, own_row_send.at[p, i], own_row_recv.at[p, i], {"tp": grid.along_row(i)})

    def own_col(p, j):
        block = arr.at[my_t, p]
        return push(block, block, own_col_send.at[p, j], own_col_recv.at[p, j], {"tp": grid.along_col(j)})

    def relay(p, i, j):
        if p % 2 == 0:
            block, peer = arr.at[grid.from_row(i), p], grid.along_col(j)
        else:
            block, peer = arr.at[grid.from_col(j), p], grid.along_row(i)
        return push(block, block, relay_send.at[p, i, j], relay_recv.at[p, i, j], {"tp": peer})

    def take(p):
        for i in range(unit):
            q = p * unit + i
            if q != home:
                out_copy(q).wait_recv()
        for i in range(1, grid_cols):
            own_row(p, i).start()
        for j in range(1, grid_rows):
            own_col(p, j).start()

    def pass_on(p):
        if p % 2 == 0:
            for i in range(1, grid_cols):
                own_row(p, i).wait_recv()
                for j in range(1, grid_rows):
                    relay(p, i, j).start()
        else:
            for j in range(1, grid_rows):
                own_col(p, j).wait_recv()
                for i in range(1, grid_cols):
                    relay(p, i, j).start()

    def gathered(p):
        if p % 2 == 0:
            for j in range(1, grid_rows):
                own_col(p, j).wait_recv()
        else:
            for i in range(1, grid_cols):
                own_row(p, i).wait_recv()
        for i in range(1, grid_cols):
            for j in range(1, grid_rows):
                relay(p, i, j).wait_recv()

    rs = Scatter(grid, part, got, comb, got2, rs_s1, rs_r1, rs_s2, rs_r2)
    tile = min(256, hidden_width)

    steps = hidden_width // tile

    def widen(g, first, last):
        pair = pl.ds(2 * g, 2)
        scale = scale_v[:, 0:1]

        @pl.loop(first, last)
        def _(f):
            cols = pl.ds(pl.multiple_of(f * tile, tile), tile)
            gate = jnp.zeros((2 * unit_rows, tile), f32)
            up = jnp.zeros((2 * unit_rows, tile), f32)
            for t in range(tp_size):
                depth = slice(t * width, (t + 1) * width)
                x = arr[t, pair].reshape(2 * unit_rows, width)
                gate += jnp.dot(x, gate_w[depth, cols], preferred_element_type=f32)
                up += jnp.dot(x, up_w[depth, cols], preferred_element_type=f32)
            gate, up = gate * scale, up * scale
            hid[:, cols] = (gate * jax.nn.sigmoid(gate) * up).astype(bf)

    def narrow(g):
        def lower(i, j):
            cols = pl.ds(pl.multiple_of(grid.at(i, j) * width, width), width)
            out = jnp.dot(hid[...], down_w[:, cols], preferred_element_type=f32).astype(bf)
            part[2 * g, rs.place(2 * g, i, j)] = out[:unit_rows]
            part[2 * g + 1, rs.place(2 * g + 1, i, j)] = out[unit_rows:]

        for i in range(1, grid_cols):
            for j in range(grid_rows):
                lower(i, j)
        rs.start(2 * g)
        for j in range(1, grid_rows):
            lower(0, j)
        rs.start(2 * g + 1)
        lower(0, 0)

    def back_copy(q):
        return push(slots.at[q], ret.at[q], back_send.at[q], back_recv.at[q], {"sp": sp_of(q)})

    def give_back(p):
        done = rs.finish(p).astype(bf)
        for i in range(unit):
            q = p * unit + i
            if q == home:
                ret[home] = done[i * cap : (i + 1) * cap]
            else:
                slots[q] = done[i * cap : (i + 1) * cap]
                back_copy(q).start()

    def stage(name, *calls):
        with jax.named_scope(name):
            for call, p in calls:
                call(p)

    def both_of(call, g):
        return (call, 2 * g), (call, 2 * g + 1)

    def expert(g, *between):
        stage(f"gathered_{g}", *both_of(gathered, g))
        with jax.named_scope(f"widen_{g}"):
            column_of(g)
            widen(g, 0, steps // 2)
        stage(f"serve_{g}", *between)
        with jax.named_scope(f"narrow_{g}"):
            widen(g, steps // 2, steps)
            narrow(g)

    for p in (7, 0, 1):
        send_out(p)
    take(6)
    with jax.named_scope("squares"):
        start_squares()
    stage("take_1", (take, 7))
    with jax.named_scope("scales"):
        send_scales()
    stage("pass_a", (pass_on, 6), (send_out, 3), (pass_on, 7))
    stage("take_b", (take, 0), (send_out, 4), (take, 1), (send_out, 5), (send_out, 2))
    stage("pass_b", (pass_on, 0), (take, 3), (pass_on, 1), (take, 2))
    for load in loads[6:]:
        load.wait()
    expert(0, (pass_on, 2), (pass_on, 3))
    stage("take_c", (take, 4))
    expert(1, (take, 5), (pass_on, 4), *both_of(rs.middle, 0))
    stage("take_d", (pass_on, 5), *both_of(give_back, 0))
    expert(2, *both_of(rs.middle, 1))
    stage("back_1", *both_of(give_back, 1))
    expert(3)
    stage("middle_2", *both_of(rs.middle, 2))
    stage("back_2", *both_of(give_back, 2))
    stage("middle_3", *both_of(rs.middle, 3))
    stage("back_3", *both_of(give_back, 3))

    with jax.named_scope("back_wait"):
        for q in others:
            back_copy(q).wait_recv()
    returned = ret[...].reshape(sp_size * cap, width)
    mixed = jnp.zeros((tokens, width), f32)
    for j, oh in enumerate((oh0, oh1)):
        mixed += weights[j] * jnp.dot(oh[...], returned, preferred_element_type=f32)
    out_ref[...] = mixed

    mix.drain()
    for u in range(pj_units):
        pj.drain(u)
    for p in range(units):
        for i in range(1, grid_cols):
            own_row(p, i).wait_send()
            for j in range(1, grid_rows):
                relay(p, i, j).wait_send()
        for j in range(1, grid_rows):
            own_col(p, j).wait_send()
        rs.drain(p)
    each(1, tp_size, lambda j: sq_copy(j).wait_send())
    for q in others:
        scale_copy(q).wait_send()
        out_copy(q).wait_send()
        back_copy(q).wait_send()


def run_layer(
    ids, chance, duo, shrink, gain, share, lane_gain, ask, keep, val, emit, skip, projection, gate, up, down, cap, heads
):
    sp_size = lax.axis_size("sp")
    tp_size = lax.axis_size("tp")
    grid_rows, grid_cols = grid_of(tp_size)
    side = max(grid_rows, grid_cols)
    tokens, model_width = skip.shape
    width = model_width // tp_size
    hidden_width = gate.shape[1]
    unit, masks = partner_order(sp_size)
    units = sp_size // unit
    rows = unit * cap
    quarter = tokens // 4
    depth = lane_gain.shape[1]
    chips = sp_size // 2
    mixer_width = heads * depth
    body = heads * depth // 2
    packed = body + heads + (-heads) % 16
    bf, f32 = jnp.bfloat16, jnp.float32
    dma = pltpu.SemaphoreType.DMA
    anywhere = pl.BlockSpec(memory_space=pl.ANY)
    vmem = pltpu.VMEM
    return pl.pallas_call(
        functools.partial(layer_kernel, sp_size, tp_size, cap, heads, depth),
        out_shape=(
            jax.ShapeDtypeStruct((tokens, width), f32),
            jax.ShapeDtypeStruct((tokens, width), bf),
        ),
        in_specs=[VMEM] * 7 + [anywhere] * 9,
        out_specs=(VMEM, VMEM),
        scratch_shapes=[
            vmem((tokens, mixer_width), bf),
            vmem((tokens, mixer_width), bf),
            vmem((tokens, mixer_width), bf),
            vmem((tokens, mixer_width), bf),
            vmem((tokens, mixer_width), f32),
            vmem((tokens, mixer_width), f32),
            vmem((tokens, mixer_width), f32),
            vmem((tokens, mixer_width), f32),
            vmem((tokens, 2 * mixer_width), bf),
            vmem((2, packed, depth), bf),
            vmem((2, packed, depth), bf),
            vmem((packed, depth), bf),
            vmem((chips, packed, depth), bf),
            vmem((body, depth), f32),
            vmem((body, depth), bf),
            vmem((body, depth), bf),
            vmem((tokens, mixer_width), bf),
            dma(()),
            dma(()),
            dma((chips,)),
            dma((chips,)),
            dma(()),
            dma(()),
            vmem(gate.shape, bf),
            vmem(up.shape, bf),
            vmem(down.shape, bf),
            vmem(projection.shape, bf),
            vmem((tokens, width), bf),
            vmem((4, tp_size, quarter, width), bf),
            vmem((4, tp_size, quarter, width), bf),
            vmem((4, side, quarter, width), bf),
            vmem((4, side, quarter, width), bf),
            vmem((128, tokens), f32),
            vmem((tp_size, 8, tokens), f32),
            vmem((sp_size, 8, 128), f32),
            vmem((sp_size, 8, 128), f32),
            vmem((2 * rows, 128), f32),
            vmem((tokens, sp_size * cap), bf),
            vmem((tokens, sp_size * cap), bf),
            vmem((sp_size, cap, width), bf),
            vmem((tp_size, units, rows, width), bf),
            vmem((units, tp_size, rows, width), bf),
            vmem((units, tp_size, rows, width), bf),
            vmem((units, side, rows, width), bf),
            vmem((units, side, rows, width), bf),
            vmem((2 * rows, hidden_width), bf),
            vmem((sp_size, cap, width), bf),
            vmem((sp_size, cap, width), bf),
            dma((9,)),
            dma((4, side)),
            dma((4, side)),
            dma((4, side)),
            dma((4, side)),
            dma((tp_size,)),
            dma((tp_size,)),
            dma((sp_size,)),
            dma((sp_size,)),
            dma((sp_size,)),
            dma((sp_size,)),
            dma((units, grid_cols)),
            dma((units, grid_cols)),
            dma((units, grid_rows)),
            dma((units, grid_rows)),
            dma((units, grid_cols, grid_rows)),
            dma((units, grid_cols, grid_rows)),
            dma((units, side)),
            dma((units, side)),
            dma((units, side)),
            dma((units, side)),
            dma((sp_size,)),
            dma((sp_size,)),
        ],
        compiler_params=pltpu.CompilerParams(
            collective_id=1, has_side_effects=True, vmem_limit_bytes=VMEM_LIMIT
        ),
    )(ids, chance, duo, shrink, gain, share, lane_gain, ask, keep, val, emit, skip, projection, gate, up, down)


def shards(
    skip_path_vectors,
    asker_raw_scores,
    retain_raw_scores,
    memory_write_entries,
    emit_switch_scores,
    retain_minimum_share,
    extra_shrink_rate,
    lane_rescale_factor,
    emit_projection_array,
    specialist_rescale_factor,
    specialist_switch_proj,
    specialist_raise_proj,
    specialist_lower_proj,
    specialist_choice_ids,
    cluster_chance,
    specialist_duo_scores,
):
    tokens = skip_path_vectors.shape[0]
    heads = extra_shrink_rate.shape[0]
    experts = lax.axis_size("sp")
    top_count = specialist_choice_ids.shape[1]
    capacity = -(-3 * tokens * top_count // (2 * experts))
    capacity = -(-capacity // 16) * 16
    routed, resid = run_layer(
        specialist_choice_ids.T,
        cluster_chance[None, :],
        specialist_duo_scores.T,
        extra_shrink_rate,
        specialist_rescale_factor[None, :],
        retain_minimum_share[None, :],
        lane_rescale_factor[None, :],
        asker_raw_scores,
        retain_raw_scores,
        memory_write_entries,
        emit_switch_scores,
        skip_path_vectors,
        emit_projection_array,
        specialist_switch_proj[0],
        specialist_raise_proj[0],
        specialist_lower_proj[0],
        capacity,
        heads,
    )
    return (resid.astype(jnp.float32) + routed).astype(jnp.bfloat16)


def solution(mesh):
    return jax.shard_map(
        shards,
        mesh=mesh,
        in_specs=(
            P("sp", None),
            P("sp", "tp"),
            P("sp", "tp"),
            P("sp", "tp"),
            P("sp", "tp"),
            P("tp"),
            P("tp", "sp"),
            P(),
            P("tp", None),
            P(),
            P("sp", None, "tp"),
            P("sp", None, "tp"),
            P("sp", "tp", None),
            P("sp", None),
            P("sp"),
            P("sp", None),
        ),
        out_specs=P("sp", "tp"),
        check_vma=False,
    )
```

```python
import functools

import jax
import jax.numpy as jnp
from jax import lax
from jax.experimental import pallas as pl
from jax.experimental.pallas import tpu as pltpu
from jax.sharding import PartitionSpec as P

EPS = 1e-06
MESH = pl.DeviceIdType.MESH
VMEM = pl.BlockSpec(memory_space=pltpu.VMEM)
VMEM_LIMIT = 56 * 1024 * 1024


def each(first, last, body):
    if last - first <= 8:
        for i in range(first, last):
            body(i)
    else:

        @pl.loop(first, last)
        def _(i):
            body(i)


def push(src, dst, send_sem, recv_sem, peer):
    return pltpu.make_async_remote_copy(
        src_ref=src,
        dst_ref=dst,
        send_sem=send_sem,
        recv_sem=recv_sem,
        device_id=peer,
        device_id_type=MESH,
    )


def grid_of(tp_size):
    cols = max(d for d in range(1, tp_size + 1) if tp_size % d == 0 and d * d <= tp_size)
    return tp_size // cols, cols


def flip(index, mask):
    bit = 1
    while bit <= mask:
        if mask & bit:
            index = index + bit * (1 - 2 * lax.rem(index // bit, 2))
        bit *= 2
    return index


def partner_order(sp_size):
    unit = sp_size // 8
    return unit, [k * unit + i for k in (2, 4, 3, 5, 6, 7, 0, 1) for i in range(unit)]


class Scatter:
    def __init__(self, grid, part, got, comb, got2, s1, r1, s2, r2):
        self.grid = grid
        self.part, self.got, self.comb, self.got2 = part, got, comb, got2
        self.s1, self.r1, self.s2, self.r2 = s1, r1, s2, r2

    def sizes(self, u):
        rows, cols = self.grid.shape
        return (cols, rows) if u % 2 == 0 else (rows, cols)

    def place(self, u, i, j):
        n1, n2 = self.sizes(u)
        return i * n2 + j if u % 2 == 0 else j * n2 + i

    def first(self, u, a):
        n1, n2 = self.sizes(u)
        peer = self.grid.along_row(a) if u % 2 == 0 else self.grid.along_col(a)
        span = pl.ds(a * n2, n2)
        return push(
            self.part.at[u, span], self.got.at[u, span], self.s1.at[u, a - 1], self.r1.at[u, a - 1], {"tp": peer}
        )

    def second(self, u, b):
        peer = self.grid.along_col(b) if u % 2 == 0 else self.grid.along_row(b)
        return push(self.comb.at[u, b], self.got2.at[u, b], self.s2.at[u, b - 1], self.r2.at[u, b - 1], {"tp": peer})

    def start(self, u):
        for a in range(1, self.sizes(u)[0]):
            self.first(u, a).start()

    def middle(self, u):
        n1, n2 = self.sizes(u)
        for a in range(1, n1):
            self.first(u, a).wait_recv()
        for b in range(1, n2):
            self.comb[u, b] = self.near_sum(u, b).astype(jnp.bfloat16)
            self.second(u, b).start()

    def near_sum(self, u, b):
        n1, n2 = self.sizes(u)
        acc = self.part[u, b].astype(jnp.float32)
        for a in range(1, n1):
            acc += self.got[u, a * n2 + b].astype(jnp.float32)
        return acc

    def finish(self, u):
        acc = self.near_sum(u, 0)
        for b in range(1, self.sizes(u)[1]):
            self.second(u, b).wait_recv()
            acc += self.got2[u, b].astype(jnp.float32)
        return acc

    def drain(self, u):
        n1, n2 = self.sizes(u)
        for a in range(1, n1):
            self.first(u, a).wait_send()
        for b in range(1, n2):
            self.second(u, b).wait_send()


class Grid:
    def __init__(self, tp_size):
        self.shape = grid_of(tp_size)
        me = lax.axis_index("tp")
        self.row, self.col = me // self.shape[1], lax.rem(me, self.shape[1])

    def at(self, i, j):
        rows, cols = self.shape
        return lax.rem(self.row + j, rows) * cols + lax.rem(self.col + i, cols)

    def along_row(self, i):
        return self.at(i, 0)

    def along_col(self, j):
        return self.at(0, j)

    def from_row(self, i):
        return self.at(self.shape[1] - i, 0)

    def from_col(self, j):
        return self.at(0, self.shape[0] - j)


def split_bf(x):
    high = x.astype(jnp.bfloat16)
    return high, (x - high.astype(jnp.float32)).astype(jnp.bfloat16)


def over_rows(a, b):
    return lax.dot_general(a, b, (((0,), (0,)), ((), ())), preferred_element_type=jnp.float32)


def over_lanes(a, b):
    return lax.dot_general(a, b, (((1,), (1,)), ((), ())), preferred_element_type=jnp.float32)


class Mixer:
    def __init__(self, heads, depth, sp_size, refs):
        (
            self.ask,
            self.keep,
            self.val,
            self.emit,
            self.key_v,
            self.cum_v,
            self.read_v,
            self.gate_v,
            self.qx_v,
            self.own,
            self.par,
            self.chip_own,
            self.chip_in,
            self.carry_f,
            self.carry_own,
            self.carry_par,
            self.mixed,
            self.pair_send,
            self.pair_recv,
            self.chip_send,
            self.chip_recv,
            self.carry_send,
            self.carry_recv,
        ) = refs
        self.heads, self.depth = heads, depth
        self.half = depth // 2
        self.body = heads * self.half
        self.chips = sp_size // 2
        self.me = lax.axis_index("sp")
        self.core = lax.rem(self.me, 2)
        self.chip = self.me // 2
        self.partner = self.me + 1 - 2 * self.core
        self.tokens = self.ask.shape[0]
        self.chunk = self.tokens // 2

    def lanes_of(self, h):
        return slice(h * self.depth, (h + 1) * self.depth)

    def rows_of(self, c):
        return slice(c * self.chunk, (c + 1) * self.chunk)

    def pair_copy(self):
        return push(self.own, self.par, self.pair_send, self.pair_recv, {"sp": self.partner})

    def chip_copy(self, d):
        return push(
            self.chip_own, self.chip_in.at[d], self.chip_send.at[d - 1], self.chip_recv.at[d - 1], {"sp": self.me + 2 * d}
        )

    def carry_copy(self):
        return push(self.carry_own, self.carry_par, self.carry_send, self.carry_recv, {"sp": self.partner})

    def states(self, share_ref, tok):
        f32, bf = jnp.float32, jnp.bfloat16
        n = self.chunk
        lower = lax.broadcasted_iota(jnp.int32, (n, n), 1) <= lax.broadcasted_iota(jnp.int32, (n, n), 0)
        lower = lower.astype(f32).astype(bf)
        for h in range(self.heads):
            lanes = self.lanes_of(h)
            share = share_ref[:, lanes]
            kept = share + (1.0 - share) * jax.nn.sigmoid(self.keep[:, lanes].astype(f32))
            key = 1.0 - kept
            decay = jnp.log(kept) + tok[:, 5 + h : 6 + h]
            self.key_v[:, lanes] = key
            parts, ends = [], []
            for c in range(2):
                rows = self.rows_of(c)
                d1, d2 = split_bf(decay[rows])
                d3 = (decay[rows] - d1.astype(f32) - d2.astype(f32)).astype(bf)
                sums = jnp.dot(lower, jnp.concatenate([d1, d2, d3], axis=1), preferred_element_type=f32)
                w = self.depth
                cum = sums[:, :w] + sums[:, w : 2 * w] + sums[:, 2 * w :]
                self.cum_v[rows, lanes] = cum
                end = cum[n - 1 : n]
                ends.append(end)
                late = jnp.concatenate(split_bf(key[rows] * jnp.exp(end - cum)), axis=1)
                state = over_rows(self.val[rows, lanes], late)
                parts.append(state[:, :w] + state[:, w:])
            self.read_v[self.rows_of(1), lanes] = parts[0]
            state = (parts[0] * jnp.exp(ends[1]) + parts[1]).astype(bf)
            total = jnp.exp(ends[0] + ends[1]).astype(bf)
            for k in range(2):
                self.own[k, h * self.half : (h + 1) * self.half] = state[k * self.half : (k + 1) * self.half]
                self.own[k, self.body + h : self.body + h + 1] = total

    def total_of(self, ref, h):
        return ref[self.body + h : self.body + h + 1].astype(jnp.float32)

    def join(self):
        f32, bf = jnp.float32, jnp.bfloat16
        self.pair_copy().wait_recv()
        own, par = self.own.at[self.core], self.par.at[self.core]
        odd = self.core == 1
        for h in range(self.heads):
            rows = slice(h * self.half, (h + 1) * self.half)
            mine, other = own[rows].astype(f32), par[rows].astype(f32)
            mine_t, other_t = self.total_of(own, h), self.total_of(par, h)
            joined = jnp.where(odd, other * mine_t + mine, mine * other_t + other)
            self.chip_own[rows] = joined.astype(bf)
            self.chip_own[self.body + h : self.body + h + 1] = (mine_t * other_t).astype(bf)
        for d in reversed(range(1, self.chips)):

            @pl.when(self.chip + d < self.chips)
            def _(d=d):
                self.chip_copy(d).start()

    def inside(self, gain_ref):
        f32, bf = jnp.float32, jnp.bfloat16
        n = self.chunk
        causal = lax.broadcasted_iota(jnp.int32, (n, n), 1) <= lax.broadcasted_iota(jnp.int32, (n, n), 0)
        for h in range(self.heads):
            lanes = self.lanes_of(h)
            first_end = None
            for c in range(2):
                rows = self.rows_of(c)
                raw = self.ask[rows, lanes].astype(f32)
                query = raw * jax.nn.sigmoid(raw)
                cum, key = self.cum_v[rows, lanes], self.key_v[rows, lanes]
                middle = cum[n // 2 - 1 : n // 2]
                q_mid = query * jnp.exp(cum - middle)
                q1, q2 = split_bf(q_mid)
                k1, k2 = split_bf(key * jnp.exp(middle - cum))
                scores = over_lanes(
                    jnp.concatenate([q1, q2, q1], axis=1), jnp.concatenate([k1, k1, k2], axis=1)
                )
                scores = jnp.where(causal, scores, 0.0)
                values = self.val[rows, lanes]
                read = jnp.dot(
                    jnp.concatenate(split_bf(scores), axis=1),
                    jnp.concatenate([values, values], axis=0),
                    preferred_element_type=f32,
                )
                q_start = query * jnp.exp(cum)
                if c == 0:
                    first_end = cum[n - 1 : n]
                else:
                    early = self.read_v[rows, lanes]
                    q_pair = jnp.concatenate(split_bf(q_start), axis=1)
                    e1 = early.astype(bf)
                    read += over_lanes(q_pair, jnp.concatenate([e1, e1], axis=1))
                    q_start = q_start * jnp.exp(first_end)
                self.read_v[rows, lanes] = read
                w = self.depth
                self.qx_v[rows, 2 * h * w : 2 * (h + 1) * w] = jnp.concatenate(split_bf(q_start), axis=1)
                raw = self.emit[rows, lanes].astype(f32)
                self.gate_v[rows, lanes] = raw * jax.nn.sigmoid(raw) * gain_ref[...]

    def carry(self):
        f32, bf = jnp.float32, jnp.bfloat16
        self.carry_f[...] = jnp.zeros_like(self.carry_f)
        shape = (1, self.depth)
        factors = [jnp.ones(shape, f32) for _ in range(self.heads)]
        for d in range(1, self.chips):
            there = self.chip >= d

            @pl.when(there)
            def _(d=d):
                self.chip_copy(d).wait_recv()
                for h in range(self.heads):
                    rows = slice(h * self.half, (h + 1) * self.half)
                    scale = jnp.ones(shape, f32)
                    for e in range(1, d):
                        scale = scale * self.total_of(self.chip_in.at[e], h)
                    self.carry_f[rows] += scale * self.chip_in[d, rows].astype(f32)

        self.carry_own[...] = self.carry_f[...].astype(bf)
        self.carry_copy().start()

    def outside(self):
        f32, bf = jnp.float32, jnp.bfloat16
        self.carry_copy().wait_recv()
        odd = self.core == 1
        for h in range(self.heads):
            lanes = self.lanes_of(h)
            rows = slice(h * self.half, (h + 1) * self.half)
            mine, other = self.carry_own[rows].astype(f32), self.carry_par[rows].astype(f32)
            low, high = jnp.where(odd, other, mine), jnp.where(odd, mine, other)
            start = jnp.concatenate([low, high], axis=0)
            before = jnp.concatenate([self.par[0, rows], self.par[1, rows]], axis=0).astype(f32)
            later = start * self.total_of(self.par.at[0], h) + before
            state = jnp.where(odd, later, start).astype(bf)
            w = self.depth
            read = self.read_v[:, lanes] + over_lanes(
                self.qx_v[:, 2 * h * w : 2 * (h + 1) * w], jnp.concatenate([state, state], axis=1)
            )
            level = jnp.mean(read * read, axis=1, keepdims=True)
            self.mixed[:, lanes] = (read * lax.rsqrt(level + EPS) * self.gate_v[:, lanes]).astype(bf)

    def drain(self):
        self.pair_copy().wait_send()
        self.carry_copy().wait_send()
        for d in range(1, self.chips):

            @pl.when(self.chip + d < self.chips)
            def _(d=d):
                self.chip_copy(d).wait_send()


def layer_kernel(
    sp_size,
    tp_size,
    cap,
    heads,
    depth,
    ids_ref,
    chance_ref,
    duo_ref,
    shrink_ref,
    gain_ref,
    share_ref,
    lane_gain_ref,
    ask_hbm,
    keep_hbm,
    val_hbm,
    emit_hbm,
    skip_hbm,
    proj_hbm,
    gate_hbm,
    up_hbm,
    down_hbm,
    out_hbm,
    mixed_v,
    resid_v,
    result_v,
    result_sem,
    *scratch,
):
    mixer_refs, scratch = scratch[:23], scratch[23:]
    (
    gate_w,
    up_w,
    down_w,
    proj_w,
    skip_v,
    pj_part,
    pj_got,
    pj_comb,
    pj_got2,
    tok_v,
    sq,
    scale_out,
    scale_in,
    scale_v,
    oh0,
    oh1,
    slots_in,
    arr,
    part,
    got,
    comb,
    got2,
    hid,
    slots,
    ret,
    load_sem,
    pj_s1,
    pj_r1,
    pj_s2,
    pj_r2,
    sq_send,
    sq_recv,
    scale_send,
    scale_recv,
    out_send,
    out_recv,
    own_row_send,
    own_row_recv,
    own_col_send,
    own_col_recv,
    relay_send,
    relay_recv,
    rs_s1,
    rs_r1,
    rs_s2,
    rs_r2,
    back_send,
    back_recv,
    ) = scratch
    my_s = lax.axis_index("sp")
    my_t = lax.axis_index("tp")
    grid = Grid(tp_size)
    grid_rows, grid_cols = grid.shape
    unit, masks = partner_order(sp_size)
    units = sp_size // unit
    unit_rows = unit * cap
    tokens, width = out_hbm.shape
    model_width, hidden_width = gate_w.shape
    bf, f32 = jnp.bfloat16, jnp.float32
    pj_units, pj_rows = pj_part.shape[0], pj_part.shape[2]

    mix = Mixer(heads, depth, sp_size, mixer_refs)
    my_cols = pl.ds(pl.multiple_of(my_t * width, width), width)
    pairs_in = (
        (keep_hbm, mix.keep),
        (val_hbm, mix.val),
        (ask_hbm, mix.ask),
        (emit_hbm, mix.emit),
        (proj_hbm, proj_w),
        (skip_hbm.at[:, my_cols], skip_v),
        (gate_hbm, gate_w),
        (up_hbm, up_w),
        (down_hbm, down_w),
    )
    loads = [pltpu.make_async_copy(src, dst, load_sem.at[i]) for i, (src, dst) in enumerate(pairs_in)]
    barrier = pltpu.get_barrier_semaphore()

    def tp_of(j):
        return lax.rem(my_t + j, tp_size)

    def sp_of(q):
        return flip(my_s, masks[q])

    others = [q for q in range(sp_size) if masks[q]]
    home = masks.index(0)

    each(
        1,
        tp_size,
        lambda j: pl.semaphore_signal(barrier, inc=1, device_id={"tp": tp_of(j)}, device_id_type=MESH),
    )
    for q in others:
        pl.semaphore_signal(barrier, inc=1, device_id={"sp": sp_of(q)}, device_id_type=MESH)
    for load in loads:
        load.start()
    tok_v[...] = jnp.zeros_like(tok_v)
    tok_v[0:2] = ids_ref[...].astype(f32)
    tok_v[2:3] = chance_ref[...]
    tok_v[3:5] = duo_ref[...]
    tok_v[5 : 5 + heads] = shrink_ref[...]
    tok = jnp.transpose(tok_v[...])
    with jax.named_scope("states"):
        loads[0].wait()
        loads[1].wait()
        mix.states(share_ref, tok)
    with jax.named_scope("barrier"):
        pl.semaphore_wait(barrier, tp_size + sp_size - 2)
    mix.pair_copy().start()
    lanes = -(-sp_size // 128) * 128
    lane = lax.broadcasted_iota(jnp.int32, (1, lanes), 1)
    base = jnp.zeros((1, lanes), f32)
    for q in range(sp_size):
        base = base + jnp.where(lane == sp_of(q), float(q * cap), 0.0)
    wide_lane = lax.broadcasted_iota(jnp.int32, (tokens, lanes), 1).astype(f32)
    mine = [(wide_lane == tok[:, j : j + 1]).astype(f32) for j in range(2)]
    row_id = lax.broadcasted_iota(jnp.int32, (tokens, tokens), 0)
    col_id = lax.broadcasted_iota(jnp.int32, (tokens, tokens), 1)
    before = (col_id < row_id).astype(f32).astype(bf)
    rank = jnp.dot(before, (mine[0] + mine[1]).astype(bf), preferred_element_type=f32) + base
    slot_ids = lax.broadcasted_iota(jnp.int32, (tokens, sp_size * cap), 1).astype(f32)
    for j, oh in enumerate((oh0, oh1)):
        spot = jnp.sum(rank * mine[j], axis=1, keepdims=True)
        oh[...] = (slot_ids == spot).astype(f32).astype(bf)
    weights = [
        tok[:, 2:3] * jax.nn.sigmoid(tok[:, 3:4] - tok[:, 4:5]),
        tok[:, 2:3] * jax.nn.sigmoid(tok[:, 4:5] - tok[:, 3:4]),
    ]

    with jax.named_scope("join"):
        mix.join()
        loads[2].wait()
        loads[3].wait()
    with jax.named_scope("inside"):
        mix.inside(lane_gain_ref)
    with jax.named_scope("carry"):
        mix.carry()
        loads[4].wait()
    with jax.named_scope("outside"):
        mix.outside()

    pj = Scatter(grid, pj_part, pj_got, pj_comb, pj_got2, pj_s1, pj_r1, pj_s2, pj_r2)

    def project(i, j):
        cols = pl.ds(pl.multiple_of(grid.at(i, j) * width, width), width)
        out = jnp.dot(mix.mixed[...], proj_w[:, cols], preferred_element_type=f32).astype(bf)
        for u in range(pj_units):
            pj_part[u, pj.place(u, i, j)] = out[u * pj_rows : (u + 1) * pj_rows]

    targets = [(i, j) for i in range(grid_cols) for j in range(grid_rows)]
    for i, j in targets:
        if i > 0:
            project(i, j)
    for i, j in targets:
        if i == 0 and j > 0:
            project(i, j)
    for u in range(pj_units):
        pj.start(u)
    project(0, 0)

    with jax.named_scope("pj_middle"):
        for u in range(pj_units):
            pj.middle(u)
        loads[5].wait()
    with jax.named_scope("pj_finish"):
        total = jnp.concatenate([pj.finish(u) for u in range(pj_units)], axis=0)
    resid = (skip_v[...].astype(f32) + total).astype(bf)
    resid_v[...] = resid
    wide = resid.astype(f32)
    def sq_copy(j):
        return push(sq.at[0], sq.at[j], sq_send.at[j - 1], sq_recv.at[j - 1], {"tp": tp_of(j)})

    row_sums = jnp.sum(wide * wide, axis=1, keepdims=True)
    sq[0] = jnp.transpose(jnp.broadcast_to(row_sums, (tokens, 128)))[:8]
    each(1, tp_size, lambda j: sq_copy(j).start())
    scaled = (wide * gain_ref[:, my_cols]).astype(bf)

    both = oh0[...] + oh1[...]
    filled = lax.dot_general(
        both, scaled, (((0,), (0,)), ((), ())), preferred_element_type=f32
    ).astype(bf)
    slots_in[...] = filled.reshape(sp_size, cap, width)
    arr[my_t, home // unit, pl.ds((home % unit) * cap, cap)] = filled[home * cap : (home + 1) * cap]

    def out_copy(q):
        dst = arr.at[my_t, q // unit, pl.ds((q % unit) * cap, cap)]
        return push(slots_in.at[q], dst, out_send.at[q], out_recv.at[q], {"sp": sp_of(q)})

    def send_out(p):
        for q in range(p * unit, (p + 1) * unit):
            if q != home:
                out_copy(q).start()

    def scale_copy(q):
        return push(
            scale_out.at[q], scale_in.at[q], scale_send.at[q], scale_recv.at[q], {"sp": sp_of(q)}
        )

    def send_scales():
        each(1, tp_size, lambda j: sq_copy(j).wait_recv())
        scale = lax.rsqrt(jnp.sum(sq[...], axis=0) / model_width + EPS)
        s1, s2 = split_bf(scale)
        s3 = (scale - s1.astype(f32) - s2.astype(f32)).astype(bf)
        picked = sum(jnp.dot(term, both, preferred_element_type=f32) for term in (s1, s2, s3))
        for q in range(sp_size):
            dst = scale_in if q == home else scale_out
            dst[q, :, 0:cap] = picked[:, q * cap : (q + 1) * cap]
        for q in others:
            scale_copy(q).start()

    def column_of(g):
        cols = []
        for q in range(2 * g * unit, 2 * (g + 1) * unit):
            if q != home:
                scale_copy(q).wait_recv()
            tall = jnp.transpose(jnp.broadcast_to(scale_in[q, 0:1], (128, 128)))
            cols.append(tall[:cap])
        scale_v[...] = jnp.concatenate(cols, axis=0)

    def own_row(p, i):
        block = arr.at[my_t, p]
        return push(block, block, own_row_send.at[p, i - 1], own_row_recv.at[p, i - 1], {"tp": grid.along_row(i)})

    def own_col(p, j):
        block = arr.at[my_t, p]
        return push(block, block, own_col_send.at[p, j - 1], own_col_recv.at[p, j - 1], {"tp": grid.along_col(j)})

    def relay(p, i, j):
        if p % 2 == 0:
            block, peer = arr.at[grid.from_row(i), p], grid.along_col(j)
        else:
            block, peer = arr.at[grid.from_col(j), p], grid.along_row(i)
        return push(block, block, relay_send.at[p, i - 1, j - 1], relay_recv.at[p, i - 1, j - 1], {"tp": peer})

    def take(p):
        for i in range(unit):
            q = p * unit + i
            if q != home:
                out_copy(q).wait_recv()
        for i in range(1, grid_cols):
            own_row(p, i).start()
        for j in range(1, grid_rows):
            own_col(p, j).start()

    def pass_on(p):
        if p % 2 == 0:
            for i in range(1, grid_cols):
                own_row(p, i).wait_recv()
                for j in range(1, grid_rows):
                    relay(p, i, j).start()
        else:
            for j in range(1, grid_rows):
                own_col(p, j).wait_recv()
                for i in range(1, grid_cols):
                    relay(p, i, j).start()

    def gathered(p):
        if p % 2 == 0:
            for j in range(1, grid_rows):
                own_col(p, j).wait_recv()
        else:
            for i in range(1, grid_cols):
                own_row(p, i).wait_recv()
        for i in range(1, grid_cols):
            for j in range(1, grid_rows):
                relay(p, i, j).wait_recv()

    rs = Scatter(grid, part, got, comb, got2, rs_s1, rs_r1, rs_s2, rs_r2)
    tile = min(256, hidden_width)

    steps = hidden_width // tile

    def widen(g, first, last):
        pair = pl.ds(2 * g, 2)
        scale = scale_v[:, 0:1]

        @pl.loop(first, last)
        def _(f):
            cols = pl.ds(pl.multiple_of(f * tile, tile), tile)
            gate = jnp.zeros((2 * unit_rows, tile), f32)
            up = jnp.zeros((2 * unit_rows, tile), f32)
            for t in range(tp_size):
                depth = slice(t * width, (t + 1) * width)
                x = arr[t, pair].reshape(2 * unit_rows, width)
                gate += jnp.dot(x, gate_w[depth, cols], preferred_element_type=f32)
                up += jnp.dot(x, up_w[depth, cols], preferred_element_type=f32)
            gate, up = gate * scale, up * scale
            hid[:, cols] = (gate * jax.nn.sigmoid(gate) * up).astype(bf)

    def narrow(g):
        def lower(i, j):
            cols = pl.ds(pl.multiple_of(grid.at(i, j) * width, width), width)
            out = jnp.dot(hid[...], down_w[:, cols], preferred_element_type=f32).astype(bf)
            part[2 * g, rs.place(2 * g, i, j)] = out[:unit_rows]
            part[2 * g + 1, rs.place(2 * g + 1, i, j)] = out[unit_rows:]

        for i in range(1, grid_cols):
            for j in range(grid_rows):
                lower(i, j)
        rs.start(2 * g)
        for j in range(1, grid_rows):
            lower(0, j)
        rs.start(2 * g + 1)
        lower(0, 0)

    def back_copy(q):
        return push(slots.at[q], ret.at[q], back_send.at[q], back_recv.at[q], {"sp": sp_of(q)})

    def give_back(p):
        done = rs.finish(p).astype(bf)
        for i in range(unit):
            q = p * unit + i
            if q == home:
                ret[home] = done[i * cap : (i + 1) * cap]
            else:
                slots[q] = done[i * cap : (i + 1) * cap]
                back_copy(q).start()

    def stage(name, *calls):
        with jax.named_scope(name):
            for call, p in calls:
                call(p)

    def both_of(call, g):
        return (call, 2 * g), (call, 2 * g + 1)

    def expert(g, *between):
        stage(f"gathered_{g}", *both_of(gathered, g))
        with jax.named_scope(f"widen_{g}"):
            column_of(g)
            widen(g, 0, steps // 2)
        stage(f"serve_{g}", *between)
        with jax.named_scope(f"narrow_{g}"):
            widen(g, steps // 2, steps)
            narrow(g)

    def combine(first, last):
        for q in range(first, last):
            if q != home:
                back_copy(q).wait_recv()
        span = slice(first * cap, last * cap)
        returned = ret[first:last].reshape((last - first) * cap, width)
        mixed = mixed_v[...] if first else resid_v[...].astype(f32)
        for j, oh in enumerate((oh0, oh1)):
            mixed += weights[j] * jnp.dot(oh[:, span], returned, preferred_element_type=f32)
        if last < sp_size:
            mixed_v[...] = mixed
        else:
            result_v[...] = mixed.astype(bf)

    for p in (7, 0, 1):
        send_out(p)
    stage("take_a", (take, 6), (take, 7))
    stage("pass_a", (pass_on, 6), (send_out, 3), (pass_on, 7))
    with jax.named_scope("scales"):
        send_scales()
    stage("take_b", (take, 0), (send_out, 4), (take, 1), (send_out, 5), (send_out, 2))
    stage("pass_b", (pass_on, 0), (take, 3), (pass_on, 1), (take, 2))
    for load in loads[6:]:
        load.wait()
    expert(0, (pass_on, 2), (pass_on, 3))
    stage("take_c", (take, 4))
    expert(1, (take, 5), (pass_on, 4), *both_of(rs.middle, 0))
    stage("take_d", (pass_on, 5), *both_of(give_back, 0))
    expert(2, *both_of(rs.middle, 1))
    stage("back_1", *both_of(give_back, 1))
    expert(3)
    stage("middle_2", *both_of(rs.middle, 2))
    with jax.named_scope("combine_a"):
        combine(0, 2 * unit)
    stage("back_2", *both_of(give_back, 2))
    stage("middle_3", *both_of(rs.middle, 3))
    with jax.named_scope("combine_b"):
        combine(2 * unit, 4 * unit)
    stage("back_3", *both_of(give_back, 3))
    with jax.named_scope("combine_c"):
        combine(4 * unit, 8 * unit)

    result_copy = pltpu.make_async_copy(result_v, out_hbm, result_sem)
    result_copy.start()
    with jax.named_scope("drain"):
        mix.drain()
        for u in range(pj_units):
            pj.drain(u)
        for p in range(units):
            for i in range(1, grid_cols):
                own_row(p, i).wait_send()
                for j in range(1, grid_rows):
                    relay(p, i, j).wait_send()
            for j in range(1, grid_rows):
                own_col(p, j).wait_send()
            rs.drain(p)
        each(1, tp_size, lambda j: sq_copy(j).wait_send())
        for q in others:
            scale_copy(q).wait_send()
            out_copy(q).wait_send()
            back_copy(q).wait_send()
    with jax.named_scope("result"):
        result_copy.wait()


def run_layer(
    ids, chance, duo, shrink, gain, share, lane_gain, ask, keep, val, emit, skip, projection, gate, up, down, cap, heads
):
    sp_size = lax.axis_size("sp")
    tp_size = lax.axis_size("tp")
    grid_rows, grid_cols = grid_of(tp_size)
    side = max(grid_rows, grid_cols)
    tokens, model_width = skip.shape
    width = model_width // tp_size
    hidden_width = gate.shape[1]
    unit, masks = partner_order(sp_size)
    units = sp_size // unit
    rows = unit * cap
    quarter = tokens // 4
    depth = lane_gain.shape[1]
    chips = sp_size // 2
    mixer_width = heads * depth
    body = heads * depth // 2
    packed = body + heads + (-heads) % 16
    bf, f32 = jnp.bfloat16, jnp.float32
    dma = pltpu.SemaphoreType.DMA
    anywhere = pl.BlockSpec(memory_space=pl.ANY)
    vmem = pltpu.VMEM
    return pl.pallas_call(
        functools.partial(layer_kernel, sp_size, tp_size, cap, heads, depth),
        out_shape=jax.ShapeDtypeStruct((tokens, width), bf),
        in_specs=[VMEM] * 7 + [anywhere] * 9,
        out_specs=anywhere,
        scratch_shapes=[
            vmem((tokens, width), f32),
            vmem((tokens, width), bf),
            vmem((tokens, width), bf),
            dma(()),
            vmem((tokens, mixer_width), bf),
            vmem((tokens, mixer_width), bf),
            vmem((tokens, mixer_width), bf),
            vmem((tokens, mixer_width), bf),
            vmem((tokens, mixer_width), f32),
            vmem((tokens, mixer_width), f32),
            vmem((tokens, mixer_width), f32),
            vmem((tokens, mixer_width), f32),
            vmem((tokens, 2 * mixer_width), bf),
            vmem((2, packed, depth), bf),
            vmem((2, packed, depth), bf),
            vmem((packed, depth), bf),
            vmem((chips, packed, depth), bf),
            vmem((body, depth), f32),
            vmem((body, depth), bf),
            vmem((body, depth), bf),
            vmem((tokens, mixer_width), bf),
            dma(()),
            dma(()),
            dma((chips - 1,)),
            dma((chips - 1,)),
            dma(()),
            dma(()),
            vmem(gate.shape, bf),
            vmem(up.shape, bf),
            vmem(down.shape, bf),
            vmem(projection.shape, bf),
            vmem((tokens, width), bf),
            vmem((4, tp_size, quarter, width), bf),
            vmem((4, tp_size, quarter, width), bf),
            vmem((4, side, quarter, width), bf),
            vmem((4, side, quarter, width), bf),
            vmem((128, tokens), f32),
            vmem((tp_size, 8, tokens), f32),
            vmem((sp_size, 8, 128), f32),
            vmem((sp_size, 8, 128), f32),
            vmem((2 * rows, 128), f32),
            vmem((tokens, sp_size * cap), bf),
            vmem((tokens, sp_size * cap), bf),
            vmem((sp_size, cap, width), bf),
            vmem((tp_size, units, rows, width), bf),
            vmem((units, tp_size, rows, width), bf),
            vmem((units, tp_size, rows, width), bf),
            vmem((units, side, rows, width), bf),
            vmem((units, side, rows, width), bf),
            vmem((2 * rows, hidden_width), bf),
            vmem((sp_size, cap, width), bf),
            vmem((sp_size, cap, width), bf),
            dma((9,)),
            dma((4, side - 1)),
            dma((4, side - 1)),
            dma((4, side - 1)),
            dma((4, side - 1)),
            dma((tp_size - 1,)),
            dma((tp_size - 1,)),
            dma((sp_size,)),
            dma((sp_size,)),
            dma((sp_size,)),
            dma((sp_size,)),
            dma((units, grid_cols - 1)),
            dma((units, grid_cols - 1)),
            dma((units, grid_rows - 1)),
            dma((units, grid_rows - 1)),
            dma((units, grid_cols - 1, grid_rows - 1)),
            dma((units, grid_cols - 1, grid_rows - 1)),
            dma((units, side - 1)),
            dma((units, side - 1)),
            dma((units, side - 1)),
            dma((units, side - 1)),
            dma((sp_size,)),
            dma((sp_size,)),
        ],
        compiler_params=pltpu.CompilerParams(
            collective_id=1, has_side_effects=True, vmem_limit_bytes=VMEM_LIMIT
        ),
    )(ids, chance, duo, shrink, gain, share, lane_gain, ask, keep, val, emit, skip, projection, gate, up, down)


def shards(
    skip_path_vectors,
    asker_raw_scores,
    retain_raw_scores,
    memory_write_entries,
    emit_switch_scores,
    retain_minimum_share,
    extra_shrink_rate,
    lane_rescale_factor,
    emit_projection_array,
    specialist_rescale_factor,
    specialist_switch_proj,
    specialist_raise_proj,
    specialist_lower_proj,
    specialist_choice_ids,
    cluster_chance,
    specialist_duo_scores,
):
    tokens = skip_path_vectors.shape[0]
    heads = extra_shrink_rate.shape[0]
    experts = lax.axis_size("sp")
    top_count = specialist_choice_ids.shape[1]
    capacity = -(-3 * tokens * top_count // (2 * experts))
    capacity = -(-capacity // 16) * 16
    return run_layer(
        specialist_choice_ids.T,
        cluster_chance[None, :],
        specialist_duo_scores.T,
        extra_shrink_rate,
        specialist_rescale_factor[None, :],
        retain_minimum_share[None, :],
        lane_rescale_factor[None, :],
        asker_raw_scores,
        retain_raw_scores,
        memory_write_entries,
        emit_switch_scores,
        skip_path_vectors,
        emit_projection_array,
        specialist_switch_proj[0],
        specialist_raise_proj[0],
        specialist_lower_proj[0],
        capacity,
        heads,
    )


def solution(mesh):
    return jax.shard_map(
        shards,
        mesh=mesh,
        in_specs=(
            P("sp", None),
            P("sp", "tp"),
            P("sp", "tp"),
            P("sp", "tp"),
            P("sp", "tp"),
            P("tp"),
            P("tp", "sp"),
            P(),
            P("tp", None),
            P(),
            P("sp", None, "tp"),
            P("sp", None, "tp"),
            P("sp", "tp", None),
            P("sp", None),
            P("sp"),
            P("sp", None),
        ),
        out_specs=P("sp", "tp"),
        check_vma=False,
    )
```
